128 devices in a mesh: ep: 64 (over z, y, x), tp: 2 (over core).
Axes of the slice: x: 4, y: 4, z: 4, core: 2. Of those that a mesh axis runs over, the one named last changes fastest.
Arguments:
- tokens: bfloat16 [1024, 2048], P('ep'), may hold values from -6 to 6
- norm_gain: bfloat16 [2048], replicated, may hold values from 0.099609375 to 1.8984375
- w_query: bfloat16 [2048, 512], P(None, 'tp'), may hold values from -0.125 to 0.125
- w_key: bfloat16 [2048, 256], P(None, 'tp'), may hold values from -0.125 to 0.125
- w_value: bfloat16 [2048, 256], P(None, 'tp'), may hold values from -0.125 to 0.125
- w_forget: bfloat16 [2048, 8], P(None, 'tp'), may hold values from -0.25 to 0.25
- w_out: bfloat16 [512, 2048], P('tp'), may hold values from -0.25 to 0.25
- cache_keys: bfloat16 [1024, 1024, 256], P('ep', None, 'tp'), may hold values from -700 to 700
- cache_values: bfloat16 [1024, 1024, 256], P('ep', None, 'tp'), may hold values from -6 to 6
- cache_gates: float32 [1024, 8, 1024], P('ep', 'tp'), as said below
- lengths: int32 [1024], P('ep'), may hold values from 1 to 1024, as said below
- ffn_gain: bfloat16 [2048], replicated, may hold values from 0.099609375 to 1.8984375
- router_w: bfloat16 [2048, 64], replicated, may hold values from -0.125 to 0.125
- routes: int32 [1024, 6], P('ep'), may hold values from 0 to 63, all different within a row; in each aligned block of 16 rows (0 to 15, 16 to 31, ...) at most 3 rows name the same one
- shared_gate: bfloat16 [2048, 512], P(None, 'tp'), may hold values from -0.125 to 0.125
- shared_up: bfloat16 [2048, 512], P(None, 'tp'), may hold values from -0.125 to 0.125
- shared_down: bfloat16 [512, 2048], P('tp'), may hold values from -0.25 to 0.25
- expert_gate: bfloat16 [64, 2048, 512], P('ep', None, 'tp'), may hold values from -0.125 to 0.125
- expert_up: bfloat16 [64, 2048, 512], P('ep', None, 'tp'), may hold values from -0.125 to 0.125
- expert_down: bfloat16 [64, 512, 2048], P('ep', 'tp'), may hold values from -0.25 to 0.25
Outputs:
- layer_out: bfloat16 [1024, 2048], P('ep')
The draws below stay inside these ranges and needn't reach their ends.
Inputs may be any that keep to these rules, and one draw needn't show every extreme that they name: `routes`: each row names 6 different experts. Among the rows of one index of ep no expert is named by more than 3 rows, and in every draw some expert is named by exactly 3 of them. `lengths`: in every draw some sequence has all 1024 positions. `cache_gates`: each row is non-increasing along the positions.
All inputs are finite; a program needn't handle non-finite values.
Results may differ from the reference program's by a relative error of at most 0.017.
Values may be sent and summed in bfloat16 or wider, within the bound.
A program may use at most 64 MiB of HBM per device.

```python
import math
import jax
import jax.numpy as jnp
import numpy as np
from jax import lax

D = 2048
QUERY_HEADS = 8
KV_HEADS = 4
HEAD_DIM = 64
SHARED_FF = 512
EXPERT_FF = 512
TOP_K = 6
SEQ_DEV = 16
CACHE_POSITIONS = 1024
SEQUENCE_TOTAL = 1024
EXPERTS = 64
CAP = 3
N_EP = 64
N_TP = 2


def draw_cache_keys(key, part):
    random_split_keys = jax.random.split(jax.random.fold_in(key, 11), 1)
    base_keys = jnp.clip(jax.random.normal(random_split_keys[0], (SEQUENCE_TOTAL, CACHE_POSITIONS, KV_HEADS * HEAD_DIM), jnp.float32), -6.0, 6.0)
    return base_keys.astype(jnp.bfloat16)


def draw_cache_gates(key, part):
    random_split_keys = jax.random.split(jax.random.fold_in(key, 23), 6)
    head_order = jax.random.permutation(random_split_keys[0], QUERY_HEADS)
    slow_heads = head_order < QUERY_HEADS // 2
    block_index = jnp.arange(SEQUENCE_TOTAL) // SEQ_DEV
    processor_multiplier = jnp.exp(jax.random.uniform(random_split_keys[1], (SEQUENCE_TOTAL // SEQ_DEV,), jnp.float32, 0.0, math.log(3.0)))[block_index]
    fast_rate = 1.0 / jnp.exp(jax.random.uniform(random_split_keys[2], (QUERY_HEADS,), jnp.float32, math.log(25.0), math.log(50.0)))
    increment_speed = jnp.where(slow_heads, 0.4 / CACHE_POSITIONS, fast_rate)
    jaggedness = jax.random.uniform(random_split_keys[3], (SEQUENCE_TOTAL, QUERY_HEADS, CACHE_POSITIONS), jnp.float32, 0.3, 1.7)
    spike_position = jax.random.uniform(random_split_keys[4], (SEQUENCE_TOTAL, QUERY_HEADS, CACHE_POSITIONS)) < 2.0 / CACHE_POSITIONS
    spike_magnitude = jnp.where(spike_position, jax.random.uniform(random_split_keys[5], (SEQUENCE_TOTAL, QUERY_HEADS, CACHE_POSITIONS), jnp.float32, 0.22, 0.69), 0.0)
    logarithm_step_count = -(increment_speed[None, :, None] * processor_multiplier[:, None, None] * jaggedness + spike_magnitude)
    return jnp.cumsum(logarithm_step_count, axis=2)


def draw_lengths(key, part):
    random_split_keys = jax.random.split(jax.random.fold_in(key, 37), 3)
    block_index = jnp.arange(SEQUENCE_TOTAL) // SEQ_DEV
    shrink = jax.random.randint(random_split_keys[0], (SEQUENCE_TOTAL // SEQ_DEV,), 0, 3)
    longest = (CACHE_POSITIONS // jnp.left_shift(1, shrink))[block_index]
    drawn = jax.random.randint(random_split_keys[1], (SEQUENCE_TOTAL,), 1, longest + 1)
    full_index = jax.random.randint(random_split_keys[2], (), 0, SEQUENCE_TOTAL)
    return jnp.where(jnp.arange(SEQUENCE_TOTAL) == full_index, CACHE_POSITIONS, drawn).astype(jnp.int32)


def block_levels(own_key, dims, shards, least, high):
    def one(position, shards_of):
        heights = jax.random.uniform(jax.random.fold_in(jax.random.fold_in(own_key, 6), position), (shards_of,), jnp.float32, least / len(shards), high / len(shards))
        return jnp.repeat(jnp.exp(heights), dims[position] // shards_of).reshape((-1,) + (1,) * (len(dims) - position - 1))

    gain = one(*shards[0])
    for cut in shards[1:]:
        gain = gain * one(*cut)
    return gain


def assign_block(stream_key, own, number, rows, count, top, most, skew):
    ranking = jax.random.permutation(stream_key, count)
    heavy_load, ordinary = shares(count, rows * top, most, skew, True), shares(count, rows * top, most, skew, False)
    places = jnp.arange(count)

    def named(sizes, offset_by):
        used = int((sizes > 0).sum())
        fixed = max(1, used // 4)
        moved = fixed + (places - fixed + offset_by * (used - fixed)) % max(1, count - fixed)
        return jnp.zeros((count,), jnp.int32).at[ranking[jnp.where(places < fixed, places, moved)]].set(jnp.asarray(sizes, jnp.int32))

    sizes = jnp.where(number % 4 == 0, named(heavy_load, number // 4), named(ordinary, number - number // 4 - 1))
    mixed = jax.random.permutation(jax.random.fold_in(own, 3), count)
    source_of, receiver = mixed[0:count // 2 * 2:2], mixed[1:count // 2 * 2:2]
    slack = jnp.minimum(sizes[source_of] - 1, most - sizes[receiver]) // 2
    slack = jnp.where((source_of == ranking[0]) | (receiver == ranking[0]) | (sizes[receiver] == 0), 0, jnp.maximum(slack, 0))
    moved = jax.random.randint(jax.random.fold_in(own, 4), (count // 2,), 0, 1 << 20) % (slack + 1)
    sizes = sizes.at[source_of].add(-moved).at[receiver].add(moved)
    items = jnp.searchsorted(jnp.cumsum(sizes), jnp.arange(rows * top), side="right").astype(jnp.int32)
    grid = items.reshape(top, rows).T
    grid = grid[jax.random.permutation(jax.random.fold_in(own, 1), rows)]
    offset_by = jax.random.randint(jax.random.fold_in(own, 2), (rows, 1), 0, top)
    return jnp.take_along_axis(grid, (jnp.arange(top)[None, :] + offset_by) % top, axis=1)


def shares(count, total, limit, lean, full):
    portions = [(1 << 20) // math.isqrt(rank ** lean) + 1 for rank in range(1, count + 1)]
    largest = limit if full else min(limit, max(-(-total // count), total * portions[0] // sum(portions)))
    least = 1 if total - largest >= count - 1 else 0
    given, spare = [largest] + [least] * (count - 1), total - largest - least * (count - 1)
    while spare > 0:
        free = [i for i in range(1, count) if given[i] < largest] or [i for i in range(1, count) if given[i] < limit]
        mass, left = sum([portions[i] for i in free]), spare
        for i in free:
            more = min(limit - given[i], max(1, left * portions[i] // mass), spare)
            given[i] = given[i] + more
            spare = spare - more
    return np.array(given)


def bell_draw(key, dims, deviation, most, cuts=(), kind=jnp.bfloat16):
    values = deviation * jax.random.normal(key, dims, jnp.float32)
    if cuts:
        values = values * block_levels(key, dims, cuts, -0.22, 0.18)
    return jnp.clip(values, -most, most).astype(kind)


def setup_inputs(seed: int = 0) -> dict:
    keys = jax.random.split(jax.random.key(seed), 21)
    tokens = bell_draw(keys[0], (SEQUENCE_TOTAL, D), 1.0, 6.0, ((0, 64),))
    norm_gain = jnp.clip(1.0 + 0.18 * jax.random.normal(keys[1], (D,), jnp.float32), 0.099609375, 1.8984375).astype(jnp.bfloat16)
    w_query = bell_draw(keys[2], (D, QUERY_HEADS * HEAD_DIM), D ** -0.5, 0.125, ((1, 2),))
    w_key = bell_draw(keys[3], (D, KV_HEADS * HEAD_DIM), D ** -0.5, 0.125, ((1, 2),))
    w_value = bell_draw(keys[4], (D, KV_HEADS * HEAD_DIM), D ** -0.5, 0.125, ((1, 2),))
    w_forget = bell_draw(keys[5], (D, QUERY_HEADS), (D // 4) ** -0.5, 0.25, ((1, 2),))
    w_out = bell_draw(keys[6], (QUERY_HEADS * HEAD_DIM, D), (QUERY_HEADS * HEAD_DIM) ** -0.5, 0.25, ((0, 2),))
    cache_keys = draw_cache_keys(jax.random.fold_in(keys[20], 71), 0)
    cache_values = bell_draw(keys[8], (SEQUENCE_TOTAL, CACHE_POSITIONS, KV_HEADS * HEAD_DIM), 1.0, 6.0, ((0, 64), (2, 2)))
    cache_gates = draw_cache_gates(jax.random.fold_in(keys[20], 71), 0)
    lengths = draw_lengths(jax.random.fold_in(keys[20], 71), 0)
    ffn_gain = jnp.clip(1.0 + 0.18 * jax.random.normal(keys[11], (D,), jnp.float32), 0.099609375, 1.8984375).astype(jnp.bfloat16)
    router_w = bell_draw(keys[12], (D, EXPERTS), D ** -0.5, 0.125)
    routes_keys = jax.random.split(jax.random.fold_in(keys[13], 1), SEQUENCE_TOTAL // SEQ_DEV)
    routes_turns = jax.random.permutation(jax.random.fold_in(keys[13], 3), SEQUENCE_TOTAL // SEQ_DEV)
    routes = jax.vmap(lambda own, number: assign_block(jax.random.fold_in(keys[13], 2), own, number, SEQ_DEV, EXPERTS, TOP_K, CAP, 2))(routes_keys, routes_turns).reshape((SEQUENCE_TOTAL, TOP_K))
    shared_gate = bell_draw(keys[14], (D, SHARED_FF), D ** -0.5, 0.125, ((1, 2),))
    shared_up = bell_draw(keys[15], (D, SHARED_FF), D ** -0.5, 0.125, ((1, 2),))
    shared_down = bell_draw(keys[16], (SHARED_FF, D), SHARED_FF ** -0.5, 0.25, ((0, 2),))
    expert_gate = bell_draw(keys[17], (EXPERTS, D, EXPERT_FF), D ** -0.5, 0.125, ((0, 64), (2, 2)))
    expert_up = bell_draw(keys[18], (EXPERTS, D, EXPERT_FF), D ** -0.5, 0.125, ((0, 64), (2, 2)))
    expert_down = bell_draw(keys[19], (EXPERTS, EXPERT_FF, D), EXPERT_FF ** -0.5, 0.25, ((0, 64), (1, 2)))
    return {"tokens": tokens, "norm_gain": norm_gain, "w_query": w_query, "w_key": w_key, "w_value": w_value, "w_forget": w_forget, "w_out": w_out, "cache_keys": cache_keys, "cache_values": cache_values, "cache_gates": cache_gates, "lengths": lengths, "ffn_gain": ffn_gain, "router_w": router_w, "routes": routes, "shared_gate": shared_gate, "shared_up": shared_up, "shared_down": shared_down, "expert_gate": expert_gate, "expert_up": expert_up, "expert_down": expert_down}


EPS = 1e-06
ROUTE_SCALE = 2.5

def norm_rows(rows, norm_gain):
    values = rows.astype(jnp.float32)
    factor = lax.rsqrt(lax.optimization_barrier(jnp.mean(values * values, axis=-1, keepdims=True)) + EPS)
    return (values * factor * norm_gain.astype(jnp.float32)).astype(jnp.bfloat16)

def parts_sum(left, right, pieces):
    width = left.shape[1] // pieces
    total_rows = jnp.zeros((left.shape[0], right.shape[1]), jnp.float32)
    for piece in range(pieces):
        partial_value = jnp.dot(left[:, piece * width:(piece + 1) * width], right[piece * width:(piece + 1) * width], preferred_element_type=jnp.float32)
        rounded = lax.optimization_barrier(partial_value.astype(jnp.bfloat16))
        total_rows = total_rows + rounded.astype(jnp.float32)
    return total_rows

def swiglu_hidden(rows, w_gate, w_up):
    gate_proj = jnp.dot(rows, w_gate, preferred_element_type=jnp.float32)
    upward = jnp.dot(rows, w_up, preferred_element_type=jnp.float32)
    return (jax.nn.silu(gate_proj) * upward).astype(jnp.bfloat16)

def route_weights(rows, router_w, chosen):
    scores = jax.nn.sigmoid(jnp.dot(rows, router_w, preferred_element_type=jnp.float32))
    picked = jnp.take_along_axis(scores, chosen, axis=1)
    return ROUTE_SCALE * picked / lax.optimization_barrier(jnp.sum(picked, axis=1, keepdims=True))

def attend_rows(inputs):
    queries, key_new, value_new, log_gate, cached_keys, cached_values, cache_gates, lengths = inputs
    seq_count = queries.shape[0]
    group_size = QUERY_HEADS // KV_HEADS
    score_scale = HEAD_DIM ** (-0.5)
    queries = queries.reshape(seq_count, KV_HEADS, group_size, HEAD_DIM).astype(jnp.float32)
    key_new = key_new.reshape(seq_count, KV_HEADS, HEAD_DIM).astype(jnp.float32)
    value_new = value_new.reshape(seq_count, KV_HEADS, HEAD_DIM).astype(jnp.float32)
    cached_keys = cached_keys.reshape(seq_count, CACHE_POSITIONS, KV_HEADS, HEAD_DIM).astype(jnp.float32)
    cached_values = cached_values.reshape(seq_count, CACHE_POSITIONS, KV_HEADS, HEAD_DIM).astype(jnp.float32)
    past_score = jnp.einsum('skgd,slkd->skgl', queries, cached_keys) * score_scale
    last_index = jnp.broadcast_to((lengths - 1).astype(jnp.int32)[:, None, None], (seq_count, QUERY_HEADS, 1))
    last_gate = jnp.take_along_axis(cache_gates, last_index, axis=2)
    gate_bias = last_gate + log_gate[:, :, None] - cache_gates
    past_score = past_score + gate_bias.reshape(seq_count, KV_HEADS, group_size, CACHE_POSITIONS)
    is_valid = jnp.arange(CACHE_POSITIONS)[None, :] < lengths[:, None]
    past_score = jnp.where(is_valid[:, None, None, :], past_score, -jnp.inf)
    self_score = jnp.einsum('skgd,skd->skg', queries, key_new) * score_scale
    peak_score = jnp.maximum(lax.optimization_barrier(jnp.max(past_score, axis=-1)), self_score)
    past_weight = jnp.exp(past_score - peak_score[..., None])
    self_weight = jnp.exp(self_score - peak_score)
    weight_sum = lax.optimization_barrier(jnp.sum(past_weight, axis=-1)) + self_weight
    past_prob = (past_weight / weight_sum[..., None]).astype(jnp.bfloat16).astype(jnp.float32)
    self_prob = (self_weight / weight_sum).astype(jnp.bfloat16).astype(jnp.float32)
    mixed_heads = jnp.einsum('skgl,slkd->skgd', past_prob, cached_values)
    mixed_heads = mixed_heads + self_prob[..., None] * value_new[:, :, None, :]
    return mixed_heads.astype(jnp.bfloat16).reshape(seq_count, QUERY_HEADS * HEAD_DIM)

def reference(tokens, norm_gain, w_query, w_key, w_value, w_forget, w_out, cache_keys, cache_values, cache_gates, lengths, ffn_gain, router_w, routes, shared_gate, shared_up, shared_down, expert_gate, expert_up, expert_down):
    normed = norm_rows(tokens, norm_gain)
    queries = jnp.dot(normed, w_query, preferred_element_type=jnp.float32).astype(jnp.bfloat16)
    keys_new = jnp.dot(normed, w_key, preferred_element_type=jnp.float32).astype(jnp.bfloat16)
    values_new = jnp.dot(normed, w_value, preferred_element_type=jnp.float32).astype(jnp.bfloat16)
    log_gate = jax.nn.log_sigmoid(jnp.dot(normed, w_forget, preferred_element_type=jnp.float32))

    def blocked(array):
        return array.reshape((N_EP, SEQ_DEV) + array.shape[1:])
    attn = lax.map(attend_rows, (blocked(queries), blocked(keys_new), blocked(values_new), blocked(log_gate), blocked(cache_keys), blocked(cache_values), blocked(cache_gates), blocked(lengths)))
    attn = attn.reshape(SEQUENCE_TOTAL, QUERY_HEADS * HEAD_DIM)
    attended = parts_sum(attn, w_out, N_TP)
    residual_rows = (tokens.astype(jnp.float32) + attended).astype(jnp.bfloat16)
    ffn_rows = norm_rows(residual_rows, ffn_gain)
    shared = parts_sum(swiglu_hidden(ffn_rows, shared_gate, shared_up), shared_down, N_TP)
    weights = route_weights(ffn_rows, router_w, routes)
    slot_count = N_EP * CAP

    def add_expert(total_rows, expert_item):
        expert_id, w_gate, w_up, w_down = expert_item
        is_routed = routes == expert_id
        chosen = jnp.any(is_routed, axis=1)
        row_index = jnp.nonzero(chosen, size=slot_count, fill_value=0)[0].astype(jnp.int32)
        live_slot = (jnp.arange(slot_count) < jnp.sum(chosen.astype(jnp.int32))).astype(jnp.float32)
        picked_rows = ffn_rows[row_index]
        answer = parts_sum(swiglu_hidden(picked_rows, w_gate, w_up), w_down, N_TP).astype(jnp.bfloat16)
        route_share = lax.optimization_barrier(jnp.sum(jnp.where(is_routed, weights, 0.0), axis=1))[row_index] * live_slot
        return (total_rows.at[row_index].add(answer.astype(jnp.float32) * route_share[:, None]), None)
    routed, _ = lax.scan(add_expert, jnp.zeros((SEQUENCE_TOTAL, D), jnp.float32), (jnp.arange(EXPERTS, dtype=jnp.int32), expert_gate, expert_up, expert_down))
    return (residual_rows.astype(jnp.float32) + shared + routed).astype(jnp.bfloat16)
```

```python
import functools

import jax
import jax.numpy as jnp
from jax import lax
from jax.experimental import pallas as pl
from jax.experimental.pallas import tpu as pltpu
from jax.sharding import PartitionSpec as P

HEAD_DIM = 64
EPS = 1e-06
ROUTE_SCALE = 2.5
CAP = 3
MESH = pl.DeviceIdType.MESH
F32 = jnp.float32
BF16 = jnp.bfloat16
HIGH = lax.Precision.HIGHEST
NT = (((1,), (1,)), ((), ()))
TN = (((0,), (0,)), ((), ()))
NN = (((1,), (0,)), ((), ()))


def dot(left, right, dims=NN, precision=None):
    return lax.dot_general(left, right, dims, precision=precision, preferred_element_type=F32)


def iota(shape, dim):
    return lax.broadcasted_iota(jnp.int32, shape, dim)


def norm_rows(values, gain):
    factor = lax.rsqrt(jnp.mean(values * values, axis=-1, keepdims=True) + EPS)
    return (values * factor * gain.astype(F32)).astype(BF16)


def silu(x):
    return x / (1.0 + jnp.exp(-x))


def log2(n):
    assert n & (n - 1) == 0
    return n.bit_length() - 1


def kernel(
    dims,
    tokens, norm_gain, w_query, w_key, w_value, w_forget, w_out, cache_keys, cache_values,
    cache_gates, lengths, ffn_gain, router_w, routes, shared_gate, shared_up, shared_down,
    expert_gate, expert_up, expert_down,
    out,
    tok, gain1, wq, wk, wv, wf, wo, kc, vc, gt, lens, gain2, rw, rt, sg, su, sd,
    eg, eu, ed, scores, heads, mine, theirs, xs, hid, lay, box_out, box_in, ret_out, ret_in,
    fin_out, fin_in, result,
    in_sem, k_sem, v_sem, att_sem, wt_send, wt_recv, go_send, go_recv, back_send, back_recv,
    fin_sem,
):
    nz, ny, nx = dims
    n_ep = nz * ny * nx
    half = n_ep // 2
    hx = nx // 2
    seqs, width = tokens.shape
    positions = cache_keys.shape[1]
    top_k = routes.shape[0]
    cols = width // 128
    rows = half * CAP
    pairs = seqs // 2
    ep = lax.axis_index("ep")
    core = lax.axis_index("tp")
    z, y, x = ep // (ny * nx), (ep // nx) % ny, ep % nx

    def peer(i, forward):
        dz = i // (ny * hx)
        dy = (i // hx) % ny
        dx = 2 * (i % hx) + (dz + dy + core) % 2
        if forward:
            pz, py, px = (z + dz) % nz, (y + dy) % ny, (x + dx) % nx
        else:
            pz, py, px = (z + nz - dz) % nz, (y + ny - dy) % ny, (x + nx - dx) % nx
        return (pz * ny + py) * nx + px

    def remote(i):
        return jnp.logical_or(core == 1, i > 0)

    barrier = pltpu.get_barrier_semaphore()

    def greet(i, carry):
        @pl.when(remote(i))
        def _():
            pl.semaphore_signal(
                barrier, inc=1, device_id=(peer(i, True), core), device_id_type=MESH
            )
        return carry

    lax.fori_loop(0, half, greet, 0)
    pl.semaphore_signal(barrier, inc=1, device_id=(ep, 1 - core), device_id_type=MESH)

    loads = {}
    order = (
        ("tok", tokens, tok), ("gain1", norm_gain, gain1), ("wq", w_query, wq), ("wk", w_key, wk),
        ("wv", w_value, wv), ("wf", w_forget, wf), ("lens", lengths, lens),
        ("gt", cache_gates, gt),
    )
    later = (
        ("wo", w_out, wo), ("gain2", ffn_gain, gain2), ("rt", routes, rt),
        ("eg", expert_gate.at[0], eg.at[0]), ("eu", expert_up.at[0], eu.at[0]),
        ("ed", expert_down.at[0], ed.at[0]),
        ("sg", shared_gate, sg), ("su", shared_up, su), ("sd", shared_down, sd),
        ("rw", router_w, rw),
    )
    slot = 0

    def load(name, src, dst):
        nonlocal slot
        loads[name] = pltpu.make_async_copy(src, dst, in_sem.at[slot])
        loads[name].start()
        slot += 1

    def ready(*names):
        for name in names:
            loads[name].wait()

    for item in order:
        load(*item)
    k_loads = []
    v_loads = []
    for p in range(pairs):
        k_loads.append(pltpu.make_async_copy(
            cache_keys.at[pl.ds(2 * p, 2)], kc.at[pl.ds(2 * p, 2)], k_sem.at[p]))
        k_loads[-1].start()
    for p in range(pairs):
        v_loads.append(pltpu.make_async_copy(
            cache_values.at[pl.ds(2 * p, 2)], vc.at[pl.ds(2 * p, 2)], v_sem.at[p]))
        v_loads[-1].start()
    for item in later:
        load(*item)

    ready("tok", "gain1")
    normed = norm_rows(tok[...].astype(F32), gain1[...])
    ready("wq")
    query = (dot(normed, wq[...]).astype(BF16).astype(F32)) * (HEAD_DIM ** -0.5)
    ready("wk")
    key_new = dot(normed, wk[...]).astype(BF16)
    ready("wv")
    value_new = dot(normed, wv[...]).astype(BF16)
    ready("wf")
    forget = dot(normed, wf[...], NT)
    forget = jnp.minimum(forget, 0.0) - jnp.log1p(jnp.exp(-jnp.abs(forget)))

    lane = iota((seqs, 128), 1)
    low = lane < 64
    q0, q1 = query[:, :128], query[:, 128:]
    q_cat = jnp.concatenate([
        jnp.where(low, q0, 0.0),
        jnp.where(low, pltpu.roll(q0, 64, 1), 0.0),
        jnp.where(low, 0.0, pltpu.roll(q1, 64, 1)),
        jnp.where(low, 0.0, q1),
    ], axis=0).astype(BF16)
    n_rows = 4 * seqs
    perm_r, perm_c = iota((n_rows, n_rows), 0), iota((n_rows, n_rows), 1)
    perm = (perm_c == (perm_r & 3) * seqs + (perm_r >> 2)).astype(F32).astype(BF16)
    spread = iota((n_rows, seqs), 1) == (iota((n_rows, seqs), 0) >> 2)
    spread_f = spread.astype(F32)
    spread_b = spread_f.astype(BF16)
    q_rows = dot(perm, q_cat)
    k_rows = dot(spread_b, key_new)
    v_rows = dot(spread_b, value_new)
    self_score = jnp.sum(q_rows * k_rows, axis=1, keepdims=True)
    gate_rows = dot(spread_f, forget, precision=HIGH)
    gate_rows = jnp.sum(
        jnp.where(iota((n_rows, 4), 1) == (iota((n_rows, 4), 0) & 3), gate_rows, 0.0),
        axis=1, keepdims=True)
    q_rows = q_rows.astype(BF16)

    ready("lens", "gt")
    first = iota((8, 128), 0) < 4
    first_pos = iota((8, positions), 0) < 4
    pos = iota((8, positions), 1)
    for p in range(pairs):
        k_loads[p].wait()
        q8 = q_rows[8 * p:8 * p + 8, :]
        zero = jnp.zeros_like(q8)
        q_pair = jnp.concatenate(
            [jnp.where(first, q8, zero), jnp.where(first, zero, q8)], axis=1)
        k_pair = jnp.concatenate([kc[2 * p], kc[2 * p + 1]], axis=1)
        s = dot(q_pair, k_pair, NT)
        g = jnp.concatenate([gt[2 * p], gt[2 * p + 1]], axis=0)
        count = jnp.where(first_pos, lens[2 * p], lens[2 * p + 1])
        last = jnp.sum(jnp.where(pos == count - 1, g, 0.0), axis=1, keepdims=True)
        s = s + ((last + gate_rows[8 * p:8 * p + 8, :]) - g)
        scores[8 * p:8 * p + 8, :] = jnp.where(pos < count, s, -jnp.inf)
    s = scores[...]
    peak = jnp.maximum(jnp.max(s, axis=1, keepdims=True), self_score)
    weight = jnp.exp(s - peak)
    self_weight = jnp.exp(self_score - peak)
    total = jnp.sum(weight, axis=1, keepdims=True) + self_weight
    scores[...] = weight / total
    self_prob = (self_weight / total).astype(BF16).astype(F32)
    for p in range(pairs):
        v_loads[p].wait()
        prob = scores[8 * p:8 * p + 8, :].astype(BF16)
        v_pair = jnp.concatenate([vc[2 * p], vc[2 * p + 1]], axis=1)
        mixed = dot(prob, v_pair)
        heads[8 * p:8 * p + 8, :] = jnp.where(first, mixed[:, :128], mixed[:, 128:])
    mixed = heads[...] + self_prob * v_rows
    row_high = (iota((n_rows, 128), 0) & 2) > 0
    lane_high = iota((n_rows, 128), 1) >= 64
    mixed = jnp.where(row_high == lane_high, mixed, 0.0).astype(BF16)
    a_cat = dot(perm, mixed, TN)
    a0, a1 = a_cat[:seqs], a_cat[seqs:2 * seqs]
    a2, a3 = a_cat[2 * seqs:3 * seqs], a_cat[3 * seqs:]
    attn = jnp.concatenate(
        [a0 + pltpu.roll(a1, 64, 1), pltpu.roll(a2, 64, 1) + a3], axis=1).astype(BF16)
    ready("wo")
    mine[...] = dot(attn, wo[...]).astype(BF16)

    pl.semaphore_wait(barrier, half + core)

    sibling = (ep, 1 - core)
    swap = pltpu.make_async_remote_copy(
        mine, theirs, att_sem.at[0], att_sem.at[1], device_id=sibling, device_id_type=MESH)
    swap.start()
    ready("eg", "eu", "ed")
    pushes = [
        pltpu.make_async_remote_copy(
            buf.at[0], buf.at[1], wt_send.at[n], wt_recv.at[n], device_id=sibling,
            device_id_type=MESH)
        for n, buf in enumerate((eg, eu, ed))
    ]
    for push in pushes:
        push.start()

    ready("gain2", "rt")
    slot_id = iota((rows, 1), 0)
    magic = -(-4096 // CAP)
    assert all((l * magic) >> 12 == l // CAP for l in range(rows))
    peer_i = (slot_id * magic) >> 12
    rank_of = slot_id - peer_i * CAP
    lhx, lny, lnx = log2(hx), log2(ny), log2(nx)
    dz = peer_i >> (lny + lhx)
    dy = (peer_i >> lhx) & (ny - 1)
    dx = 2 * (peer_i & (hx - 1)) + ((dz + dy + core) & 1)
    expert_of = (
        (((z + dz) & (nz - 1)) << (lny + lnx)) + (((y + dy) & (ny - 1)) << lnx)
        + ((x + dx) & (nx - 1)))
    routed_to = rt[...]
    marks = jnp.zeros((rows, seqs), F32)
    marks_all = jnp.zeros((n_ep, seqs), F32)
    all_experts = iota((n_ep, seqs), 0)
    for k in range(top_k):
        marks = marks + (routed_to[k:k + 1, :] == expert_of).astype(F32)
        marks_all = marks_all + (routed_to[k:k + 1, :] == all_experts).astype(F32)
    earlier = (iota((seqs, seqs), 0) < iota((seqs, seqs), 1)).astype(F32)
    rank = dot(marks.astype(BF16), earlier.astype(BF16))
    pick = jnp.where(rank == rank_of.astype(F32), marks, 0.0)
    pick_b = pick.astype(BF16)

    swap.wait_recv()
    residual = (
        tok[...].astype(F32) + (mine[...].astype(F32) + theirs[...].astype(F32))).astype(BF16)
    ffn_rows = norm_rows(residual.astype(F32), gain2[...])

    for j in range(cols // 2):
        part = dot(pick_b, ffn_rows[:, 256 * j:256 * j + 256])
        lay[pl.ds(2 * j, rows, stride=cols), :] = part[:, :128]
        lay[pl.ds(2 * j + 1, rows, stride=cols), :] = part[:, 128:]
    box_out[...] = lay[...].astype(BF16).reshape(box_out.shape)

    def go(i):
        return pltpu.make_async_remote_copy(
            box_out.at[i], box_in.at[i], go_send.at[i], go_recv.at[i],
            device_id=(peer(i, True), core), device_id_type=MESH)

    def back(i):
        return pltpu.make_async_remote_copy(
            ret_out.at[i], ret_in.at[i], back_send.at[i], back_recv.at[i],
            device_id=(peer(i, False), core), device_id_type=MESH)

    def each(action):
        def step(i, carry):
            @pl.when(remote(i))
            def _():
                action(i)
            return carry
        lax.fori_loop(0, half, step, 0)

    each(lambda i: go(i).start())

    @pl.when(core == 0)
    def _():
        box_in[0] = box_out[0]

    ready("rw")
    chance = dot(rw[...], ffn_rows, NT)
    chance = marks_all / (1.0 + jnp.exp(-chance))
    share = ROUTE_SCALE * chance / jnp.sum(chance, axis=0, keepdims=True)
    to_slot = (iota((rows, n_ep), 1) == expert_of).astype(F32)
    slot_w = dot(to_slot, share, precision=HIGH) * pick
    slot_hi = slot_w.astype(BF16)
    slot_lo = (slot_w - slot_hi.astype(F32)).astype(BF16)
    ready("sg", "su", "sd")
    shared_h = (silu(dot(ffn_rows, sg[...])) * dot(ffn_rows, su[...])).astype(BF16)
    shared = dot(shared_h, sd[...]).astype(BF16)
    fin_out[...] = shared.astype(F32)

    each(lambda i: go(i).wait_recv())
    lay[...] = box_in[...].reshape(lay.shape).astype(F32)
    for j in range(cols):
        xs[:, 128 * j:128 * j + 128] = lay[pl.ds(j, rows, stride=cols), :].astype(BF16)
    hidden_w = eg.shape[2]
    for part in range(2):
        if part == 1:
            for push in pushes:
                push.wait_recv()
        gate = dot(xs[...], eg[part])
        up = dot(xs[...], eu[part])
        hid[:, hidden_w * part:hidden_w * (part + 1)] = (silu(gate) * up).astype(BF16)
    for j in range(cols // 2):
        down = ed[:, :, 256 * j:256 * j + 256].reshape(2 * hidden_w, 256)
        answer = dot(hid[...], down)
        lay[pl.ds(2 * j, rows, stride=cols), :] = answer[:, :128]
        lay[pl.ds(2 * j + 1, rows, stride=cols), :] = answer[:, 128:]
    ret_out[...] = lay[...].astype(BF16).reshape(ret_out.shape)
    each(lambda i: back(i).start())

    @pl.when(core == 0)
    def _():
        ret_in[0] = ret_out[0]

    each(lambda i: back(i).wait_recv())
    lay[...] = ret_in[...].reshape(lay.shape).astype(F32)
    for j in range(cols):
        answer = lay[pl.ds(j, rows, stride=cols), :].astype(BF16)
        part = dot(slot_hi, answer, TN) + dot(slot_lo, answer, TN)
        fin_out[:, 128 * j:128 * j + 128] += part

    finish = pltpu.make_async_remote_copy(
        fin_out, fin_in, fin_sem.at[0], fin_sem.at[1], device_id=sibling, device_id_type=MESH)
    finish.start()
    finish.wait_recv()
    result[...] = (residual.astype(F32) + (fin_out[...] + fin_in[...])).astype(BF16)
    write = pltpu.make_async_copy(result, out, in_sem.at[0])
    write.start()
    finish.wait_send()
    swap.wait_send()
    for push in pushes:
        push.wait_send()
    each(lambda i: go(i).wait_send())
    each(lambda i: back(i).wait_send())
    write.wait()


def split_dims(n):
    return {64: (4, 4, 4), 4: (1, 2, 2), 8: (2, 2, 2)}[n]


def per_device(
    tokens, norm_gain, w_query, w_key, w_value, w_forget, w_out, cache_keys, cache_values,
    cache_gates, lengths, ffn_gain, router_w, routes, shared_gate, shared_up, shared_down,
    expert_gate, expert_up, expert_down,
):
    seqs, width = tokens.shape
    n_ep = lax.axis_size("ep")
    half = n_ep // 2
    rows = half * CAP
    cols = width // 128
    positions = cache_keys.shape[1]
    ff = expert_gate.shape[2]
    any_spec = pl.BlockSpec(memory_space=pl.ANY)
    operands = (
        tokens, norm_gain.reshape(1, width), w_query, w_key, w_value, w_forget.T, w_out,
        cache_keys, cache_values, cache_gates, lengths, ffn_gain.reshape(1, width), router_w.T,
        routes.T, shared_gate, shared_up, shared_down, expert_gate, expert_up, expert_down,
    )
    vmem = pltpu.VMEM
    dma = pltpu.SemaphoreType.DMA

    def like(index):
        return vmem(operands[index].shape, operands[index].dtype)

    scratch = [
        like(0), like(1), like(2), like(3), like(4), like(5), like(6), like(7), like(8), like(9),
        pltpu.SMEM(lengths.shape, jnp.int32), like(11), like(12), like(13), like(14), like(15),
        like(16),
        vmem((2, width, ff), BF16), vmem((2, width, ff), BF16), vmem((2, ff, width), BF16),
        vmem((4 * seqs, positions), F32), vmem((4 * seqs, 128), F32),
        vmem((seqs, width), BF16), vmem((seqs, width), BF16),
        vmem((rows, width), BF16), vmem((rows, 2 * ff), BF16), vmem((rows * cols, 128), F32),
        vmem((half, CAP * cols, 128), BF16), vmem((half, CAP * cols, 128), BF16),
        vmem((half, CAP * cols, 128), BF16), vmem((half, CAP * cols, 128), BF16),
        vmem((seqs, width), F32), vmem((seqs, width), F32), vmem((seqs, width), BF16),
        dma((18,)), dma((seqs // 2,)), dma((seqs // 2,)), dma((2,)), dma((3,)), dma((3,)),
        dma((half,)), dma((half,)), dma((half,)), dma((half,)), dma((2,)),
    ]
    return pl.pallas_call(
        functools.partial(kernel, split_dims(n_ep)),
        out_shape=jax.ShapeDtypeStruct((seqs, width), BF16),
        in_specs=[any_spec] * len(operands),
        out_specs=any_spec,
        scratch_shapes=scratch,
        compiler_params=pltpu.CompilerParams(
            collective_id=0, has_side_effects=True, vmem_limit_bytes=62 * 1024 * 1024),
    )(*operands)


def solution(mesh):
    placed = (
        P("ep", None),
        P(),
        P(None, "tp"),
        P(None, "tp"),
        P(None, "tp"),
        P(None, "tp"),
        P("tp", None),
        P("ep", None, "tp"),
        P("ep", None, "tp"),
        P("ep", "tp", None),
        P("ep"),
        P(),
        P(),
        P("ep", None),
        P(None, "tp"),
        P(None, "tp"),
        P("tp", None),
        P("ep", None, "tp"),
        P("ep", None, "tp"),
        P("ep", "tp", None),
    )
    return jax.shard_map(
        per_device, mesh=mesh, in_specs=placed, out_specs=P("ep", None), check_vma=False
    )
```

```python
import functools

import jax
import jax.numpy as jnp
from jax import lax
from jax.experimental import pallas as pl
from jax.experimental.pallas import tpu as pltpu
from jax.sharding import PartitionSpec as P

HEAD_DIM = 64
EPS = 1e-06
ROUTE_SCALE = 2.5
CAP = 3
GROUPS = 2
MESH = pl.DeviceIdType.MESH
F32 = jnp.float32
BF16 = jnp.bfloat16
HIGH = lax.Precision.HIGHEST
NT = (((1,), (1,)), ((), ()))
TN = (((0,), (0,)), ((), ()))
NN = (((1,), (0,)), ((), ()))


def dot(left, right, dims=NN, precision=None):
    return lax.dot_general(left, right, dims, precision=precision, preferred_element_type=F32)


def iota(shape, dim):
    return lax.broadcasted_iota(jnp.int32, shape, dim)


def norm_rows(values, gain):
    factor = lax.rsqrt(jnp.mean(values * values, axis=-1, keepdims=True) + EPS)
    return (values * factor * gain.astype(F32)).astype(BF16)


def silu(x):
    return x / (1.0 + jnp.exp(-x))


class Phases:
    def __init__(self):
        self.scope = None

    def __call__(self, name=None):
        if self.scope is not None:
            self.scope.__exit__(None, None, None)
        self.scope = jax.named_scope(name) if name else None
        if self.scope is not None:
            self.scope.__enter__()


def peer_tables(dims):
    nz, ny, nx = dims
    tables = ([], [])
    for dz in range(nz):
        for dy in range(ny):
            for dx in range(nx):
                far = min(dz, nz - dz) + min(dy, ny - dy) + min(dx, nx - dx)
                tables[dx % 2].append((-far, dz, dy, dx))
    return [[entry[1:] for entry in sorted(table)] for table in tables]


def log2(n):
    assert n & (n - 1) == 0
    return n.bit_length() - 1


def kernel(
    dims,
    tokens, norm_gain, w_query, w_key, w_value, w_forget, w_out, cache_keys, cache_values,
    cache_gates, lengths, ffn_gain, router_w, routes, shared_gate, shared_up, shared_down,
    expert_gate, expert_up, expert_down,
    out,
    tok, gain1, wq, wk, wv, wf, wo, kc, vc, gt, lens, gain2, rw, rt, sg, su, sd,
    eg, eu, ed, scores, heads, mine, theirs, xs, hid, lay, box_out, box_in, ret_out, ret_in,
    total_rows, fin_out, fin_in,
    in_sem, k_sem, v_sem, att_sem, wt_send, wt_recv, go_send, go_recv, back_send, back_recv,
    fin_sem,
):
    nz, ny, nx = dims
    n_ep = nz * ny * nx
    half = n_ep // 2
    group = half // GROUPS
    seqs, width = tokens.shape
    positions = cache_keys.shape[1]
    top_k = routes.shape[0]
    cols = width // 128
    rows = half * CAP
    g_rows = group * CAP
    pairs = seqs // 2
    ep = lax.axis_index("ep")
    core = lax.axis_index("tp")
    z, y, x = ep // (ny * nx), (ep // nx) % ny, ep % nx
    tables = peer_tables(dims)

    def by_core(first, second):
        return first if first == second else first + core * (second - first)

    def peer(i, forward):
        dz, dy, dx = (by_core(a, b) for a, b in zip(tables[0][i], tables[1][i]))
        if forward:
            pz, py, px = (z + dz) % nz, (y + dy) % ny, (x + dx) % nx
        else:
            pz, py, px = (z + nz - dz) % nz, (y + ny - dy) % ny, (x + nx - dx) % nx
        return (pz * ny + py) * nx + px

    def each(numbers, action):
        for i in numbers:
            if i < half - 1:
                action(i)
            else:
                pl.when(core == 1)(functools.partial(action, i))

    phase = Phases()
    phase("loads")
    loads = {}
    order = (
        ("tok", tokens, tok), ("gain1", norm_gain, gain1), ("wq", w_query, wq), ("wk", w_key, wk),
        ("wv", w_value, wv), ("wf", w_forget, wf), ("lens", lengths, lens),
        ("rt", routes, rt), ("gt", cache_gates, gt),
    )
    later = (
        ("wo", w_out, wo), ("gain2", ffn_gain, gain2),
        ("eg", expert_gate.at[0], eg.at[0]), ("eu", expert_up.at[0], eu.at[0]),
        ("ed", expert_down.at[0], ed.at[0]),
        ("sg", shared_gate, sg), ("su", shared_up, su), ("sd", shared_down, sd),
        ("rw", router_w, rw),
    )
    slot = 0

    def load(name, src, dst):
        nonlocal slot
        loads[name] = pltpu.make_async_copy(src, dst, in_sem.at[slot])
        loads[name].start()
        slot += 1

    def ready(*names):
        for name in names:
            loads[name].wait()

    for item in order:
        load(*item)
    k_loads = [
        pltpu.make_async_copy(
            cache_keys.at[pl.ds(2 * p, 2)], kc.at[pl.ds(2 * p, 2)], k_sem.at[p])
        for p in range(pairs)
    ]
    v_loads = [
        pltpu.make_async_copy(
            cache_values.at[pl.ds(2 * p, 2)], vc.at[pl.ds(2 * p, 2)], v_sem.at[p])
        for p in range(pairs)
    ]
    for p in range(pairs // 2):
        k_loads[p].start()

    phase("greet")
    barrier = pltpu.get_barrier_semaphore()

    def greet(i):
        pl.semaphore_signal(
            barrier, inc=1, device_id=(peer(i, True), core), device_id_type=MESH)

    each(range(half), greet)
    pl.semaphore_signal(barrier, inc=1, device_id=(ep, 1 - core), device_id_type=MESH)

    phase("slots")
    ready("rt")
    slot_id = iota((rows, 1), 0)
    magic = -(-4096 // CAP)
    assert all((l * magic) >> 12 == l // CAP for l in range(rows))
    peer_i = (slot_id * magic) >> 12
    rank_of = slot_id - peer_i * CAP
    lny, lnx = log2(ny), log2(nx)

    def packed(entry):
        return (entry[0] << (lny + lnx)) + (entry[1] << lnx) + entry[2]

    code = jnp.zeros_like(slot_id)
    for i in range(half):
        code = jnp.where(
            peer_i == i, by_core(packed(tables[0][i]), packed(tables[1][i])), code)
    dz, dy, dx = code >> (lny + lnx), (code >> lnx) & (ny - 1), code & (nx - 1)
    expert_of = (
        (((z + dz) & (nz - 1)) << (lny + lnx)) + (((y + dy) & (ny - 1)) << lnx)
        + ((x + dx) & (nx - 1)))
    routed_to = rt[...]
    marks = jnp.zeros((rows, seqs), F32)
    marks_all = jnp.zeros((n_ep, seqs), F32)
    all_experts = iota((n_ep, seqs), 0)
    for k in range(top_k):
        marks = marks + (routed_to[k:k + 1, :] == expert_of).astype(F32)
        marks_all = marks_all + (routed_to[k:k + 1, :] == all_experts).astype(F32)
    earlier = (iota((seqs, seqs), 0) < iota((seqs, seqs), 1)).astype(F32)
    rank = dot(marks.astype(BF16), earlier.astype(BF16))
    pick = jnp.where(rank == rank_of.astype(F32), marks, 0.0)
    pick_b = pick.astype(BF16)
    to_slot = (iota((rows, n_ep), 1) == expert_of).astype(F32)

    phase("project")
    ready("tok", "gain1")
    for p in range(pairs // 2, pairs):
        k_loads[p].start()
    normed = norm_rows(tok[...].astype(F32), gain1[...].reshape(1, width))
    ready("wq")
    query = (dot(normed, wq[...]).astype(BF16).astype(F32)) * (HEAD_DIM ** -0.5)
    ready("wk")
    key_new = dot(normed, wk[...]).astype(BF16)
    ready("wv")
    value_new = dot(normed, wv[...]).astype(BF16)
    ready("wf")
    forget = dot(normed, wf[...], NT)
    forget = jnp.minimum(forget, 0.0) - jnp.log1p(jnp.exp(-jnp.abs(forget)))

    lane = iota((seqs, 128), 1)
    low = lane < 64
    q0, q1 = query[:, :128], query[:, 128:]
    q_cat = jnp.concatenate([
        jnp.where(low, q0, 0.0),
        jnp.where(low, pltpu.roll(q0, 64, 1), 0.0),
        jnp.where(low, 0.0, pltpu.roll(q1, 64, 1)),
        jnp.where(low, 0.0, q1),
    ], axis=0).astype(BF16)
    n_rows = 4 * seqs
    perm_r, perm_c = iota((n_rows, n_rows), 0), iota((n_rows, n_rows), 1)
    perm = (perm_c == (perm_r & 3) * seqs + (perm_r >> 2)).astype(F32).astype(BF16)
    spread = iota((n_rows, seqs), 1) == (iota((n_rows, seqs), 0) >> 2)
    spread_f = spread.astype(F32)
    spread_b = spread_f.astype(BF16)
    q_rows = dot(perm, q_cat)
    k_rows = dot(spread_b, key_new)
    v_rows = dot(spread_b, value_new)
    self_score = jnp.sum(q_rows * k_rows, axis=1, keepdims=True)
    gate_rows = dot(spread_f, forget, precision=HIGH)
    gate_rows = jnp.sum(
        jnp.where(iota((n_rows, 4), 1) == (iota((n_rows, 4), 0) & 3), gate_rows, 0.0),
        axis=1, keepdims=True)
    q_rows = q_rows.astype(BF16)

    phase("score")
    phase("k_wait")
    for p in range(pairs):
        k_loads[p].wait()
        v_loads[p].start()
    phase("score2")
    ready("lens", "gt")
    first = iota((8, 128), 0) < 4
    first_pos = iota((8, positions), 0) < 4
    pos = iota((8, positions), 1)
    for p in range(pairs):
        q8 = q_rows[8 * p:8 * p + 8, :]
        zero = jnp.zeros_like(q8)
        q_pair = jnp.concatenate(
            [jnp.where(first, q8, zero), jnp.where(first, zero, q8)], axis=1)
        k_pair = jnp.concatenate([kc[2 * p], kc[2 * p + 1]], axis=1)
        s = dot(q_pair, k_pair, NT)
        g = jnp.concatenate([gt[2 * p], gt[2 * p + 1]], axis=0)
        count = jnp.where(first_pos, lens[2 * p], lens[2 * p + 1])
        last = jnp.sum(jnp.where(pos == count - 1, g, 0.0), axis=1, keepdims=True)
        s = s + ((last + gate_rows[8 * p:8 * p + 8, :]) - g)
        scores[8 * p:8 * p + 8, :] = jnp.where(pos < count, s, -jnp.inf)
    phase("softmax")
    s = scores[...]
    peak = jnp.maximum(jnp.max(s, axis=1, keepdims=True), self_score)
    weight = jnp.exp(s - peak)
    self_weight = jnp.exp(self_score - peak)
    total = jnp.sum(weight, axis=1, keepdims=True) + self_weight
    scores[...] = weight / total
    self_prob = (self_weight / total).astype(BF16).astype(F32)
    phase("values")
    for item in later:
        load(*item)
    phase("v_wait")
    for p in range(pairs):
        v_loads[p].wait()
    phase("values2")
    for p in range(pairs):
        prob = scores[8 * p:8 * p + 8, :].astype(BF16)
        v_pair = jnp.concatenate([vc[2 * p], vc[2 * p + 1]], axis=1)
        mixed = dot(prob, v_pair)
        heads[8 * p:8 * p + 8, :] = jnp.where(first, mixed[:, :128], mixed[:, 128:])
    mixed = heads[...] + self_prob * v_rows
    row_high = (iota((n_rows, 128), 0) & 2) > 0
    lane_high = iota((n_rows, 128), 1) >= 64
    mixed = jnp.where(row_high == lane_high, mixed, 0.0).astype(BF16)
    a_cat = dot(perm, mixed, TN)
    a0, a1 = a_cat[:seqs], a_cat[seqs:2 * seqs]
    a2, a3 = a_cat[2 * seqs:3 * seqs], a_cat[3 * seqs:]
    attn = jnp.concatenate(
        [a0 + pltpu.roll(a1, 64, 1), pltpu.roll(a2, 64, 1) + a3], axis=1).astype(BF16)
    ready("wo")
    mine[...] = dot(attn, wo[...]).astype(BF16)

    phase("barrier")
    pl.semaphore_wait(barrier, half + core)

    phase("swap_start")
    sibling = (ep, 1 - core)
    swap = pltpu.make_async_remote_copy(
        mine, theirs, att_sem.at[0], att_sem.at[1], device_id=sibling, device_id_type=MESH)
    swap.start()
    ready("gain2")
    phase("swap_wait")
    swap.wait_recv()
    phase("norm2")
    residual = (
        tok[...].astype(F32) + (mine[...].astype(F32) + theirs[...].astype(F32))).astype(BF16)
    ffn_rows = norm_rows(residual.astype(F32), gain2[...].reshape(1, width))

    phase("pack")

    def go(i):
        return pltpu.make_async_remote_copy(
            box_out.at[i], box_in.at[i], go_send.at[i], go_recv.at[i],
            device_id=(peer(i, True), core), device_id_type=MESH)

    def back(i):
        return pltpu.make_async_remote_copy(
            ret_out.at[i], ret_in.at[i], back_send.at[i], back_recv.at[i],
            device_id=(peer(i, False), core), device_id_type=MESH)

    def members(g):
        return range(g * group, (g + 1) * group)

    def lines(g, j):
        return pl.ds(g * g_rows * cols + j, g_rows, stride=cols)

    def whole(g):
        return pl.ds(g * g_rows * cols, g_rows * cols)

    for g in range(GROUPS):
        chosen = pick_b[g * g_rows:(g + 1) * g_rows]
        for j in range(cols // 2):
            part = dot(chosen, ffn_rows[:, 256 * j:256 * j + 256])
            lay[lines(g, 2 * j), :] = part[:, :128]
            lay[lines(g, 2 * j + 1), :] = part[:, 128:]
        box_out[pl.ds(g * group, group)] = lay[whole(g), :].astype(BF16).reshape(
            group, CAP * cols, 128)
        each(members(g), lambda i: go(i).start())

    @pl.when(core == 0)
    def _():
        box_in[half - 1] = box_out[half - 1]

    ready("eg", "eu", "ed")
    pushes = [
        pltpu.make_async_remote_copy(
            buf.at[0], buf.at[1], wt_send.at[n], wt_recv.at[n], device_id=sibling,
            device_id_type=MESH)
        for n, buf in enumerate((eg, eu, ed))
    ]
    for push in pushes:
        push.start()

    phase("shared")
    ready("rw")
    chance = dot(rw[...], ffn_rows, NT)
    chance = marks_all / (1.0 + jnp.exp(-chance))
    share = ROUTE_SCALE * chance / jnp.sum(chance, axis=0, keepdims=True)
    slot_w = dot(to_slot, share, precision=HIGH) * pick
    slot_hi = slot_w.astype(BF16).astype(F32)
    slot_w = jnp.concatenate([slot_hi, slot_w - slot_hi], axis=1)
    mix = [
        jnp.transpose(slot_w[g * g_rows:(g + 1) * g_rows]).astype(BF16) for g in range(GROUPS)
    ]
    ready("sg", "su", "sd")
    shared_h = (silu(dot(ffn_rows, sg[...])) * dot(ffn_rows, su[...])).astype(BF16)
    total_rows[...] = dot(shared_h, sd[...])

    hidden_w = eg.shape[2]
    for g in range(GROUPS):
        phase(f"go_wait{g}")
        each(members(g), lambda i: go(i).wait_recv())
        phase(f"unpack{g}")
        lay[whole(g), :] = box_in[pl.ds(g * group, group)].reshape(
            g_rows * cols, 128).astype(F32)
        for j in range(cols):
            xs[:, 128 * j:128 * j + 128] = lay[lines(g, j), :].astype(BF16)
        phase(f"ffn_in{g}")
        for part in range(2):
            if part == 1 and g == 0:
                for push in pushes:
                    push.wait_recv()
            gate = dot(xs[...], eg[part])
            up = dot(xs[...], eu[part])
            hid[:, hidden_w * part:hidden_w * (part + 1)] = (silu(gate) * up).astype(BF16)
        phase(f"ffn_out{g}")
        for j in range(cols // 2):
            down = ed[:, :, 256 * j:256 * j + 256].reshape(2 * hidden_w, 256)
            answer = dot(hid[...], down)
            lay[lines(g, 2 * j), :] = answer[:, :128]
            lay[lines(g, 2 * j + 1), :] = answer[:, 128:]
        ret_out[pl.ds(g * group, group)] = lay[whole(g), :].astype(BF16).reshape(
            group, CAP * cols, 128)
        phase(f"back_start{g}")
        each(members(g), lambda i: back(i).start())

    @pl.when(core == 0)
    def _():
        ret_in[half - 1] = ret_out[half - 1]

    for g in range(GROUPS):
        phase(f"back_wait{g}")
        each(members(g), lambda i: back(i).wait_recv())
        phase(f"combine{g}")
        lay[whole(g), :] = ret_in[pl.ds(g * group, group)].reshape(
            g_rows * cols, 128).astype(F32)
        for j in range(cols // 2):
            answer = jnp.concatenate(
                [lay[lines(g, 2 * j), :], lay[lines(g, 2 * j + 1), :]], axis=1).astype(BF16)
            part = dot(mix[g], answer)
            part = total_rows[:, 256 * j:256 * j + 256] + (part[:seqs] + part[seqs:])
            if g < GROUPS - 1:
                total_rows[:, 256 * j:256 * j + 256] = part
            else:
                fin_out[:, 256 * j:256 * j + 256] = part.astype(BF16)

    phase("finish")
    finish = pltpu.make_async_remote_copy(
        fin_out, fin_in, fin_sem.at[0], fin_sem.at[1], device_id=sibling, device_id_type=MESH)
    finish.start()
    swap.wait_send()
    for push in pushes:
        push.wait_send()
    each(range(half), lambda i: go(i).wait_send())
    each(range(half), lambda i: back(i).wait_send())
    finish.wait_recv()
    phase("result")
    out[...] = (
        residual.astype(F32) + (fin_out[...].astype(F32) + fin_in[...].astype(F32))).astype(BF16)
    finish.wait_send()
    phase()


def split_dims(n):
    return {64: (4, 4, 4), 4: (1, 2, 2), 8: (2, 2, 2)}[n]


def per_device(
    tokens, norm_gain, w_query, w_key, w_value, w_forget, w_out, cache_keys, cache_values,
    cache_gates, lengths, ffn_gain, router_w, routes, shared_gate, shared_up, shared_down,
    expert_gate, expert_up, expert_down,
):
    seqs, width = tokens.shape
    n_ep = lax.axis_size("ep")
    half = n_ep // 2
    rows = half * CAP
    cols = width // 128
    positions = cache_keys.shape[1]
    ff = expert_gate.shape[2]
    any_spec = pl.BlockSpec(memory_space=pl.ANY)
    operands = (
        tokens, norm_gain, w_query, w_key, w_value, w_forget.T, w_out,
        cache_keys, cache_values, cache_gates, lengths, ffn_gain, router_w.T,
        routes.T, shared_gate, shared_up, shared_down, expert_gate, expert_up, expert_down,
    )
    vmem = pltpu.VMEM
    dma = pltpu.SemaphoreType.DMA

    def like(index):
        return vmem(operands[index].shape, operands[index].dtype)

    scratch = [
        like(0), like(1), like(2), like(3), like(4), like(5), like(6), like(7), like(8), like(9),
        pltpu.SMEM(lengths.shape, jnp.int32), like(11), like(12), like(13), like(14), like(15),
        like(16),
        vmem((2, width, ff), BF16), vmem((2, width, ff), BF16), vmem((2, ff, width), BF16),
        vmem((4 * seqs, positions), F32), vmem((4 * seqs, 128), F32),
        vmem((seqs, width), BF16), vmem((seqs, width), BF16),
        vmem((rows // GROUPS, width), BF16), vmem((rows // GROUPS, 2 * ff), BF16), vmem((rows * cols, 128), F32),
        vmem((half, CAP * cols, 128), BF16), vmem((half, CAP * cols, 128), BF16),
        vmem((half, CAP * cols, 128), BF16), vmem((half, CAP * cols, 128), BF16),
        vmem((seqs, width), F32), vmem((seqs, width), BF16), vmem((seqs, width), BF16),
        dma((18,)), dma((seqs // 2,)), dma((seqs // 2,)), dma((2,)), dma((3,)), dma((3,)),
        dma((half,)), dma((half,)), dma((half,)), dma((half,)), dma((2,)),
    ]
    return pl.pallas_call(
        functools.partial(kernel, split_dims(n_ep)),
        out_shape=jax.ShapeDtypeStruct((seqs, width), BF16),
        in_specs=[any_spec] * len(operands),
        out_specs=pl.BlockSpec(memory_space=pltpu.VMEM),
        scratch_shapes=scratch,
        compiler_params=pltpu.CompilerParams(
            collective_id=0, has_side_effects=True, vmem_limit_bytes=62 * 1024 * 1024),
    )(*operands)


def solution(mesh):
    placed = (
        P("ep", None),
        P(),
        P(None, "tp"),
        P(None, "tp"),
        P(None, "tp"),
        P(None, "tp"),
        P("tp", None),
        P("ep", None, "tp"),
        P("ep", None, "tp"),
        P("ep", "tp", None),
        P("ep"),
        P(),
        P(),
        P("ep", None),
        P(None, "tp"),
        P(None, "tp"),
        P("tp", None),
        P("ep", None, "tp"),
        P("ep", None, "tp"),
        P("ep", "tp", None),
    )
    return jax.shard_map(
        per_device, mesh=mesh, in_specs=placed, out_specs=P("ep", None), check_vma=False
    )
```

```python
import functools

import jax
import jax.numpy as jnp
from jax import lax
from jax.experimental import pallas as pl
from jax.experimental.pallas import tpu as pltpu
from jax.sharding import PartitionSpec as P

HEAD_DIM = 64
EPS = 1e-06
ROUTE_SCALE = 2.5
CAP = 3
GROUPS = 2
SLOTS = 9
SPLIT = 4
FAR_TURNS = {5: (1,), 4: (1, 1, 0), 1: (0,)}
MESH = pl.DeviceIdType.MESH
F32 = jnp.float32
BF16 = jnp.bfloat16
HIGH = lax.Precision.HIGHEST
NT = (((1,), (1,)), ((), ()))
TN = (((0,), (0,)), ((), ()))
NN = (((1,), (0,)), ((), ()))


def dot(left, right, dims=NN, precision=None):
    return lax.dot_general(left, right, dims, precision=precision, preferred_element_type=F32)


def iota(shape, dim):
    return lax.broadcasted_iota(jnp.int32, shape, dim)


def norm_rows(values, gain):
    factor = lax.rsqrt(jnp.mean(values * values, axis=-1, keepdims=True) + EPS)
    return (values * factor * gain.astype(F32)).astype(BF16)


def silu(x):
    return x / (1.0 + jnp.exp(-x))


class Phases:
    def __init__(self):
        self.scope = None

    def __call__(self, name=None):
        if self.scope is not None:
            self.scope.__exit__(None, None, None)
        self.scope = jax.named_scope(name) if name else None
        if self.scope is not None:
            self.scope.__enter__()


def peer_tables(dims):
    nz, ny, nx = dims

    def far(entry):
        return sum(min(d, n - d) for d, n in zip(entry, dims))

    def negative(entry):
        return tuple((n - d) % n for d, n in zip(entry, dims))

    entries = [(dz, dy, dx) for dz in range(nz) for dy in range(ny) for dx in range(nx)]
    half = len(entries) // 2
    entries = sorted(entries[1:], key=lambda entry: (-far(entry), sum(entry), entry))
    tables = ([(0, 0, 0)], [])
    seen = {}
    for entry in entries:
        pair = sorted({entry, negative(entry)})
        if len(pair) == 2 and entry == pair[0]:
            count = seen.get(far(entry), 0)
            seen[far(entry)] = count + 1
            turns = FAR_TURNS.get(far(entry), (0, 1))
            core = turns[count % len(turns)]
            tables[core].extend(pair)
    for entry in entries:
        if entry == negative(entry):
            tables[int(len(tables[1]) < half)].append(entry)
    for table in tables:
        table.sort(key=lambda entry: -far(entry))
    assert len(tables[0]) == len(tables[1])
    return tables


def log2(n):
    assert n & (n - 1) == 0
    return n.bit_length() - 1


def kernel(
    dims,
    tokens, norm_gain, w_query, w_key, w_value, w_forget, w_out, cache_keys, cache_values,
    cache_gates, lengths, ffn_gain, router_w, routes, shared_gate, shared_up, shared_down,
    expert_gate, expert_up, expert_down,
    out_residual, out_mine, out_theirs,
    tok, gain1, wq, wk, wv, wf, wo, kc, vc, gt, lens, gain2, rw, rt, sg, su, sd,
    eg, eu, ed, scores, heads, fanned, mine, theirs, kept, xs, hid, lay, box_out, box_in, ret_out, ret_in,
    total_rows, fin_out,
    in_sem, k_sem, v_sem, att_sem, wt_send, wt_recv, go_send, go_recv, back_send, back_recv,
    fin_sem,
):
    nz, ny, nx = dims
    n_ep = nz * ny * nx
    half = n_ep // 2
    group = half // GROUPS
    seqs, width = tokens.shape
    positions = cache_keys.shape[1]
    top_k = routes.shape[0]
    cols = width // 128
    rows = half * CAP
    g_rows = group * CAP
    pairs = seqs // 2
    ep = lax.axis_index("ep")
    core = lax.axis_index("tp")
    z, y, x = ep // (ny * nx), (ep // nx) % ny, ep % nx
    tables = peer_tables(dims)

    def by_core(first, second):
        return first if first == second else first + core * (second - first)

    def peer(i, forward):
        dz, dy, dx = (by_core(a, b) for a, b in zip(tables[0][i], tables[1][i]))
        if forward:
            pz, py, px = (z + dz) % nz, (y + dy) % ny, (x + dx) % nx
        else:
            pz, py, px = (z + nz - dz) % nz, (y + ny - dy) % ny, (x + nx - dx) % nx
        return (pz * ny + py) * nx + px

    def each(numbers, action):
        for i in numbers:
            if i < half - 1:
                action(i)
            else:
                pl.when(core == 1)(functools.partial(action, i))

    phase = Phases()
    phase("loads")
    loads = {}
    order = (
        ("rt", routes, rt), ("tok", tokens, tok), ("gain1", norm_gain, gain1),
        ("lens", lengths, lens), ("wf", w_forget, wf), ("wq", w_query, wq), ("wk", w_key, wk),
        ("wv", w_value, wv), ("gt", cache_gates, gt),
    )
    later = (
        ("rw", router_w, rw), ("gain2", ffn_gain, gain2),
        ("eg", expert_gate.at[0], eg.at[0]), ("eu", expert_up.at[0], eu.at[0]),
        ("ed", expert_down.at[0], ed.at[0]),
        ("sg", shared_gate, sg), ("su", shared_up, su), ("sd", shared_down, sd),
    )
    slot = 0

    def load(name, src, dst):
        nonlocal slot
        loads[name] = pltpu.make_async_copy(src, dst, in_sem.at[slot % SLOTS])
        loads[name].start()
        slot += 1

    def ready(*names):
        for name in names:
            loads[name].wait()

    for item in order:
        load(*item)
    step = seqs // SPLIT

    def cache_copy(src, dst, sem, n):
        return pltpu.make_async_copy(
            src.at[pl.ds(n * step, step)], dst.at[pl.ds(n * step, step)], sem.at[n])

    k_loads = [cache_copy(cache_keys, kc, k_sem, n) for n in range(SPLIT)]
    v_loads = [cache_copy(cache_values, vc, v_sem, n) for n in range(SPLIT)]
    for copy in k_loads:
        copy.start()

    phase("greet")
    barrier = pltpu.get_barrier_semaphore()

    def greet(i):
        pl.semaphore_signal(
            barrier, inc=1, device_id=(peer(i, True), core), device_id_type=MESH)

    each(range(half), greet)
    pl.semaphore_signal(barrier, inc=1, device_id=(ep, 1 - core), device_id_type=MESH)

    phase("slots")
    ready("rt")
    slot_id = iota((rows, 1), 0)
    magic = -(-4096 // CAP)
    assert all((l * magic) >> 12 == l // CAP for l in range(rows))
    peer_i = (slot_id * magic) >> 12
    rank_of = slot_id - peer_i * CAP
    lny, lnx = log2(ny), log2(nx)

    def packed(entry):
        return (entry[0] << (lny + lnx)) + (entry[1] << lnx) + entry[2]

    code = jnp.zeros_like(slot_id)
    for i in range(half):
        code = jnp.where(
            peer_i == i, by_core(packed(tables[0][i]), packed(tables[1][i])), code)
    dz, dy, dx = code >> (lny + lnx), (code >> lnx) & (ny - 1), code & (nx - 1)
    expert_of = (
        (((z + dz) & (nz - 1)) << (lny + lnx)) + (((y + dy) & (ny - 1)) << lnx)
        + ((x + dx) & (nx - 1)))
    routed_to = rt[...]
    marks = jnp.zeros((rows, seqs), F32)
    marks_all = jnp.zeros((n_ep, seqs), F32)
    all_experts = iota((n_ep, seqs), 0)
    for k in range(top_k):
        marks = marks + (routed_to[k:k + 1, :] == expert_of).astype(F32)
        marks_all = marks_all + (routed_to[k:k + 1, :] == all_experts).astype(F32)
    earlier = (iota((seqs, seqs), 0) < iota((seqs, seqs), 1)).astype(F32)
    rank = dot(marks.astype(BF16), earlier.astype(BF16))
    pick = jnp.where(rank == rank_of.astype(F32), marks, 0.0)
    pick_b = pick.astype(BF16)
    to_slot = (iota((rows, n_ep), 1) == expert_of).astype(F32)

    phase("project")
    ready("tok", "gain1", "wq", "wk", "wv", "wf", "lens", "gt")
    for copy in v_loads[:SPLIT // 2]:
        copy.start()
    normed = norm_rows(tok[...].astype(F32), gain1[...].reshape(1, width))
    query = (dot(normed, wq[...]).astype(BF16).astype(F32)) * (HEAD_DIM ** -0.5)
    key_new = dot(normed, wk[...]).astype(BF16).astype(F32)
    value_new = dot(normed, wv[...]).astype(BF16).astype(F32)
    forget = dot(normed, wf[...], NT)
    forget = jnp.minimum(forget, 0.0) - jnp.log1p(jnp.exp(-jnp.abs(forget)))

    n_rows = 4 * seqs
    low = iota((seqs, 128), 1) < 64
    q0, q1 = query[:, :128], query[:, 128:]
    by_head = (
        jnp.where(low, q0, 0.0), jnp.where(low, pltpu.roll(q0, 64, 1), 0.0),
        jnp.where(low, 0.0, pltpu.roll(q1, 64, 1)), jnp.where(low, 0.0, q1),
    )
    for h in range(4):
        of_head = pl.ds(h, seqs, stride=4)
        fanned[0, of_head, :] = by_head[h]
        fanned[1, of_head, :] = key_new
        fanned[2, of_head, :] = value_new
        fanned[3, of_head, :] = jnp.broadcast_to(forget[:, h:h + 1], (seqs, 128))
    q_rows = fanned[0]
    v_rows = fanned[2]
    self_score = jnp.sum(q_rows * fanned[1], axis=1, keepdims=True)
    gate_rows = fanned[3][:, :1]
    q_rows = q_rows.astype(BF16)

    first = iota((8, 128), 0) < 4
    first_pos = iota((8, positions), 0) < 4
    pos = iota((8, positions), 1)
    for p in range(pairs):
        if p == 0:
            phase("k_wait0")
            for copy in k_loads[:SPLIT // 2]:
                copy.wait()
            for copy in v_loads[SPLIT // 2:]:
                copy.start()
            load("wo", w_out, wo)
            phase("score0")
        if p == pairs // 2:
            phase("k_wait1")
            for copy in k_loads[SPLIT // 2:]:
                copy.wait()
            phase("score1")
        q8 = q_rows[8 * p:8 * p + 8, :]
        zero = jnp.zeros_like(q8)
        q_pair = jnp.concatenate(
            [jnp.where(first, q8, zero), jnp.where(first, zero, q8)], axis=1)
        k_pair = jnp.concatenate([kc[2 * p], kc[2 * p + 1]], axis=1)
        s = dot(q_pair, k_pair, NT)
        g = jnp.concatenate([gt[2 * p], gt[2 * p + 1]], axis=0)
        count = jnp.where(first_pos, lens[2 * p], lens[2 * p + 1])
        last = jnp.sum(jnp.where(pos == count - 1, g, 0.0), axis=1, keepdims=True)
        s = s + ((last + gate_rows[8 * p:8 * p + 8, :]) - g)
        scores[8 * p:8 * p + 8, :] = jnp.where(pos < count, s, -jnp.inf)
    phase("softmax")
    s = scores[...]
    peak = jnp.maximum(jnp.max(s, axis=1, keepdims=True), self_score)
    weight = jnp.exp(s - peak)
    self_weight = jnp.exp(self_score - peak)
    total = jnp.sum(weight, axis=1, keepdims=True) + self_weight
    scores[...] = weight / total
    self_prob = (self_weight / total).astype(BF16).astype(F32)
    for p in range(pairs):
        if p == 0:
            phase("v_wait0")
            for copy in v_loads[:SPLIT // 2]:
                copy.wait()
            for item in later:
                load(*item)
            phase("values0")
        if p == pairs // 2:
            phase("v_wait1")
            for copy in v_loads[SPLIT // 2:]:
                copy.wait()
            ready("wo")
            phase("values1")
        prob = scores[8 * p:8 * p + 8, :].astype(BF16)
        v_pair = jnp.concatenate([vc[2 * p], vc[2 * p + 1]], axis=1)
        mixed = dot(prob, v_pair)
        heads[8 * p:8 * p + 8, :] = jnp.where(first, mixed[:, :128], mixed[:, 128:])
    heads[...] = heads[...] + self_prob * v_rows
    a0, a1, a2, a3 = (
        heads[pl.ds(h, seqs, stride=4), :].astype(BF16).astype(F32) for h in range(4))
    attn = jnp.concatenate([
        jnp.where(low, a0, pltpu.roll(a1, 64, 1)), jnp.where(low, pltpu.roll(a2, 64, 1), a3),
    ], axis=1).astype(BF16)
    mine[...] = dot(attn, wo[...]).astype(BF16)

    phase("barrier")
    pl.semaphore_wait(barrier, half + core)

    phase("swap_start")
    sibling = (ep, 1 - core)
    swap = pltpu.make_async_remote_copy(
        mine, theirs, att_sem.at[0], att_sem.at[1], device_id=sibling, device_id_type=MESH)
    swap.start()
    ready("gain2")
    phase("swap_wait")
    swap.wait_recv()
    phase("norm2")
    residual = (
        tok[...].astype(F32) + (mine[...].astype(F32) + theirs[...].astype(F32))).astype(BF16)
    kept[...] = residual
    keep = pltpu.make_async_copy(kept, out_residual, fin_sem.at[2])
    keep.start()
    ffn_rows = norm_rows(residual.astype(F32), gain2[...].reshape(1, width))

    phase("pack")

    def lot(i):
        return GROUPS if i == half - 1 else i // group

    def landed(g, src, dst, send, recv, wait):
        count = group - (g == GROUPS - 1)
        if count:
            part = pl.ds(g * group, count)
            wait(pltpu.make_async_remote_copy(
                src.at[part], dst.at[part], send.at[g], recv.at[g],
                device_id=sibling, device_id_type=MESH))
        if g == GROUPS - 1:
            @pl.when(core == 1)
            def _():
                wait(pltpu.make_async_remote_copy(
                    src.at[half - 1], dst.at[half - 1], send.at[GROUPS], recv.at[GROUPS],
                    device_id=sibling, device_id_type=MESH))

    def go_landed(g, wait):
        landed(g, box_out, box_in, go_send, go_recv, wait)

    def back_landed(g, wait):
        landed(g, ret_out, ret_in, back_send, back_recv, wait)

    def go(i):
        return pltpu.make_async_remote_copy(
            box_out.at[i], box_in.at[i], go_send.at[lot(i)], go_recv.at[lot(i)],
            device_id=(peer(i, True), core), device_id_type=MESH)

    def back(i):
        return pltpu.make_async_remote_copy(
            ret_out.at[i], ret_in.at[i], back_send.at[lot(i)], back_recv.at[lot(i)],
            device_id=(peer(i, False), core), device_id_type=MESH)

    def members(g):
        return range(g * group, (g + 1) * group)

    def lines(g, j):
        return pl.ds(g * g_rows * cols + j, g_rows, stride=cols)

    def whole(g):
        return pl.ds(g * g_rows * cols, g_rows * cols)

    for g in range(GROUPS):
        chosen = pick_b[g * g_rows:(g + 1) * g_rows]
        for j in range(cols // 2):
            part = dot(chosen, ffn_rows[:, 256 * j:256 * j + 256])
            lay[lines(g, 2 * j), :] = part[:, :128]
            lay[lines(g, 2 * j + 1), :] = part[:, 128:]
        box_out[pl.ds(g * group, group)] = lay[whole(g), :].astype(BF16).reshape(
            group, CAP * cols, 128)
        each(members(g), lambda i: go(i).start())

    @pl.when(core == 0)
    def _():
        box_in[half - 1] = box_out[half - 1]

    ready("eg", "eu", "ed")
    pushes = [
        pltpu.make_async_remote_copy(
            buf.at[0], buf.at[1], wt_send.at[n], wt_recv.at[n], device_id=sibling,
            device_id_type=MESH)
        for n, buf in enumerate((eg, eu, ed))
    ]
    for push in pushes:
        push.start()

    phase("shared")
    ready("rw")
    chance = dot(rw[...], ffn_rows, NT)
    chance = marks_all / (1.0 + jnp.exp(-chance))
    share = ROUTE_SCALE * chance / jnp.sum(chance, axis=0, keepdims=True)
    slot_w = dot(to_slot, share, precision=HIGH) * pick
    slot_hi = slot_w.astype(BF16).astype(F32)
    slot_w = jnp.concatenate([slot_hi, slot_w - slot_hi], axis=1)
    mix = [
        jnp.transpose(slot_w[g * g_rows:(g + 1) * g_rows]).astype(BF16) for g in range(GROUPS)
    ]
    ready("sg", "su", "sd")
    shared_h = (silu(dot(ffn_rows, sg[...])) * dot(ffn_rows, su[...])).astype(BF16)
    total_rows[...] = dot(shared_h, sd[...])

    hidden_w = eg.shape[2]
    phase("push_wait")
    for push in pushes:
        push.wait_recv()
    for g in range(GROUPS):
        phase(f"go_wait{g}")
        go_landed(g, lambda copy: copy.wait_recv())
        phase(f"unpack{g}")
        lay[whole(g), :] = box_in[pl.ds(g * group, group)].reshape(
            g_rows * cols, 128).astype(F32)
        for j in range(cols):
            xs[:, 128 * j:128 * j + 128] = lay[lines(g, j), :].astype(BF16)
        phase(f"ffn_in{g}")
        for part in range(2):
            gate = dot(xs[...], eg[part])
            up = dot(xs[...], eu[part])
            hid[:, hidden_w * part:hidden_w * (part + 1)] = (silu(gate) * up).astype(BF16)
        phase(f"ffn_out{g}")
        for j in range(cols // 2):
            down = ed[:, :, 256 * j:256 * j + 256].reshape(2 * hidden_w, 256)
            answer = dot(hid[...], down)
            lay[lines(g, 2 * j), :] = answer[:, :128]
            lay[lines(g, 2 * j + 1), :] = answer[:, 128:]
        ret_out[pl.ds(g * group, group)] = lay[whole(g), :].astype(BF16).reshape(
            group, CAP * cols, 128)
        phase(f"back_start{g}")
        each(members(g), lambda i: back(i).start())

    @pl.when(core == 0)
    def _():
        ret_in[half - 1] = ret_out[half - 1]

    for g in range(GROUPS):
        phase(f"back_wait{g}")
        back_landed(g, lambda copy: copy.wait_recv())
        phase(f"combine{g}")
        lay[whole(g), :] = ret_in[pl.ds(g * group, group)].reshape(
            g_rows * cols, 128).astype(F32)
        for j in range(cols // 2):
            answer = jnp.concatenate(
                [lay[lines(g, 2 * j), :], lay[lines(g, 2 * j + 1), :]], axis=1).astype(BF16)
            part = dot(mix[g], answer)
            part = total_rows[:, 256 * j:256 * j + 256] + (part[:seqs] + part[seqs:])
            if g < GROUPS - 1:
                total_rows[:, 256 * j:256 * j + 256] = part
            else:
                fin_out[:, 256 * j:256 * j + 256] = part.astype(BF16)

    phase("finish")
    finish = pltpu.make_async_remote_copy(
        fin_out, out_theirs, fin_sem.at[0], fin_sem.at[1], device_id=sibling,
        device_id_type=MESH)
    finish.start()
    own = pltpu.make_async_copy(fin_out, out_mine, fin_sem.at[3])
    own.start()
    swap.wait_send()
    for push in pushes:
        push.wait_send()
    for g in range(GROUPS):
        go_landed(g, lambda copy: copy.wait_send())
        back_landed(g, lambda copy: copy.wait_send())
    keep.wait()
    own.wait()
    finish.wait_send()
    finish.wait_recv()
    phase()


def split_dims(n):
    return {64: (4, 4, 4), 4: (1, 2, 2), 8: (2, 2, 2)}[n]


def per_device(
    tokens, norm_gain, w_query, w_key, w_value, w_forget, w_out, cache_keys, cache_values,
    cache_gates, lengths, ffn_gain, router_w, routes, shared_gate, shared_up, shared_down,
    expert_gate, expert_up, expert_down,
):
    seqs, width = tokens.shape
    n_ep = lax.axis_size("ep")
    half = n_ep // 2
    rows = half * CAP
    cols = width // 128
    positions = cache_keys.shape[1]
    ff = expert_gate.shape[2]
    any_spec = pl.BlockSpec(memory_space=pl.ANY)
    operands = (
        tokens, norm_gain, w_query, w_key, w_value, w_forget.T, w_out,
        cache_keys, cache_values, cache_gates, lengths, ffn_gain, router_w.T,
        routes.T, shared_gate, shared_up, shared_down, expert_gate, expert_up, expert_down,
    )
    vmem = pltpu.VMEM
    dma = pltpu.SemaphoreType.DMA

    def like(index):
        return vmem(operands[index].shape, operands[index].dtype)

    scratch = [
        like(0), like(1), like(2), like(3), like(4), like(5), like(6), like(7), like(8), like(9),
        pltpu.SMEM(lengths.shape, jnp.int32), like(11), like(12), like(13), like(14), like(15),
        like(16),
        vmem((2, width, ff), BF16), vmem((2, width, ff), BF16), vmem((2, ff, width), BF16),
        vmem((4 * seqs, positions), F32), vmem((4 * seqs, 128), F32),
        vmem((4, 4 * seqs, 128), F32),
        vmem((seqs, width), BF16), vmem((seqs, width), BF16), vmem((seqs, width), BF16),
        vmem((rows // GROUPS, width), BF16), vmem((rows // GROUPS, 2 * ff), BF16), vmem((rows * cols, 128), F32),
        vmem((half, CAP * cols, 128), BF16), vmem((half, CAP * cols, 128), BF16),
        vmem((half, CAP * cols, 128), BF16), vmem((half, CAP * cols, 128), BF16),
        vmem((seqs, width), F32), vmem((seqs, width), BF16),
        dma((SLOTS,)), dma((SPLIT,)), dma((SPLIT,)), dma((2,)), dma((3,)), dma((3,)),
        dma((GROUPS + 1,)), dma((GROUPS + 1,)), dma((GROUPS + 1,)), dma((GROUPS + 1,)), dma((4,)),
    ]
    residual, own, other = pl.pallas_call(
        functools.partial(kernel, split_dims(n_ep)),
        out_shape=[jax.ShapeDtypeStruct((seqs, width), BF16)] * 3,
        in_specs=[any_spec] * len(operands),
        out_specs=[any_spec] * 3,
        scratch_shapes=scratch,
        compiler_params=pltpu.CompilerParams(
            collective_id=0, has_side_effects=True, vmem_limit_bytes=62 * 1024 * 1024),
    )(*operands)
    return (residual.astype(F32) + (own.astype(F32) + other.astype(F32))).astype(BF16)


def solution(mesh):
    placed = (
        P("ep", None),
        P(),
        P(None, "tp"),
        P(None, "tp"),
        P(None, "tp"),
        P(None, "tp"),
        P("tp", None),
        P("ep", None, "tp"),
        P("ep", None, "tp"),
        P("ep", "tp", None),
        P("ep"),
        P(),
        P(),
        P("ep", None),
        P(None, "tp"),
        P(None, "tp"),
        P("tp", None),
        P("ep", None, "tp"),
        P("ep", None, "tp"),
        P("ep", "tp", None),
    )
    return jax.shard_map(
        per_device, mesh=mesh, in_specs=placed, out_specs=P("ep", None), check_vma=False
    )
```

```python
import functools

import jax
import jax.numpy as jnp
from jax import lax
from jax.experimental import pallas as pl
from jax.experimental.pallas import tpu as pltpu
from jax.sharding import PartitionSpec as P

HEAD_DIM = 64
EPS = 1e-06
ROUTE_SCALE = 2.5
CAP = 3
Z_STEP = 2
SLOTS = 9
SPLIT = 4
MESH = pl.DeviceIdType.MESH
F32 = jnp.float32
BF16 = jnp.bfloat16
HIGH = lax.Precision.HIGHEST
NT = (((1,), (1,)), ((), ()))
TN = (((0,), (0,)), ((), ()))
NN = (((1,), (0,)), ((), ()))


def dot(left, right, dims=NN, precision=None):
    return lax.dot_general(left, right, dims, precision=precision, preferred_element_type=F32)


def iota(shape, dim):
    return lax.broadcasted_iota(jnp.int32, shape, dim)


def norm_rows(values, gain):
    factor = lax.rsqrt(jnp.mean(values * values, axis=-1, keepdims=True) + EPS)
    return (values * factor * gain.astype(F32)).astype(BF16)


def silu(x):
    return x / (1.0 + jnp.exp(-x))


class Phases:
    def __init__(self):
        self.scope = None

    def __call__(self, name=None):
        if self.scope is not None:
            self.scope.__exit__(None, None, None)
        self.scope = jax.named_scope(name) if name else None
        if self.scope is not None:
            self.scope.__enter__()


def plane_tables(dims):
    ny, nx = dims[1:]

    def far(entry):
        return min(entry[0], ny - entry[0]) + min(entry[1], nx - entry[1])

    entries = [(dy, dx) for dy in range(ny) for dx in range(nx)]
    entries.sort(key=lambda entry: (-far(entry), entry))
    half = len(entries) // 2
    pairs, single = [], []
    for entry in entries:
        other = ((ny - entry[0]) % ny, (nx - entry[1]) % nx)
        if other == entry:
            single.append(entry)
        elif entry < other:
            pairs.append([entry, other])
    cut = len(pairs) // 2
    second = sum(pairs[:cut], [])
    fill = half - len(second)
    tables = (sum(pairs[cut:], []) + single[fill:], second + single[:fill])
    for table in tables:
        table.sort(key=lambda entry: -far(entry))
    assert len(tables[0]) == len(tables[1])
    return tables


def log2(n):
    assert n & (n - 1) == 0
    return n.bit_length() - 1


def kernel(
    dims,
    tokens, norm_gain, w_query, w_key, w_value, w_forget, w_out, cache_keys, cache_values,
    cache_gates, lengths, ffn_gain, router_w, routes, shared_gate, shared_up, shared_down,
    expert_gate, expert_up, expert_down,
    out_residual, out_mine, out_theirs,
    tok, gain1, wq, wk, wv, wf, wo, kc, vc, gt, lens, gain2, rw, rt, sg, su, sd,
    eg, eu, ed, scores, heads, fanned, mine, theirs, kept, xs, hid, lay, box_out, box_in, ret_out, ret_in,
    total_rows, fin_out,
    in_sem, k_sem, v_sem, att_sem, wt_send, wt_recv, go_send, go_recv, back_send, back_recv,
    fin_sem,
):
    nz, ny, nx = dims
    n_ep = nz * ny * nx
    half = n_ep // 2
    block = half // nz
    seqs, width = tokens.shape
    positions = cache_keys.shape[1]
    top_k = routes.shape[0]
    cols = width // 128
    rows = half * CAP
    b_rows = block * CAP
    z_step = min(Z_STEP, nz)
    pairs = seqs // 2
    ep = lax.axis_index("ep")
    core = lax.axis_index("tp")
    z, y, x = ep // (ny * nx), (ep // nx) % ny, ep % nx
    tables = plane_tables(dims)

    def by_core(first, second):
        return first if first == second else first + core * (second - first)

    def peer(dz, k, forward):
        dy, dx = (by_core(a, b) for a, b in zip(tables[0][k], tables[1][k]))
        if forward:
            pz, py, px = (z + dz) % nz, (y + dy) % ny, (x + dx) % nx
        else:
            pz, py, px = (z + nz - dz) % nz, (y + ny - dy) % ny, (x + nx - dx) % nx
        return (pz * ny + py) * nx + px

    def each(dz, action):
        for k in range(block - 1):
            action(k)
        here = jnp.logical_and(core == 0, dz == 0)
        pl.when(jnp.logical_not(here))(functools.partial(action, block - 1))

    phase = Phases()
    phase("loads")
    loads = {}
    order = (
        ("rt", routes, rt), ("tok", tokens, tok), ("gain1", norm_gain, gain1),
    )
    later = (
        ("rw", router_w, rw), ("gain2", ffn_gain, gain2),
        ("eg", expert_gate.at[0], eg.at[0]), ("eu", expert_up.at[0], eu.at[0]),
        ("ed", expert_down.at[0], ed.at[0]),
        ("sg", shared_gate, sg), ("su", shared_up, su), ("sd", shared_down, sd),
    )
    slot = 0

    def load(name, src, dst, pieces=1):
        nonlocal slot
        sem = in_sem.at[slot % SLOTS]
        loads[name] = pltpu.make_async_copy(src, dst, sem)
        size = src.shape[0] // pieces
        for n in range(pieces):
            part = pl.ds(n * size, size)
            if pieces == 1:
                loads[name].start()
            else:
                pltpu.make_async_copy(src.at[part], dst.at[part], sem).start()
        slot += 1

    def ready(*names):
        for name in names:
            loads[name].wait()

    for item in order:
        load(*item)
    load("wq", w_query, wq, 4)
    load("lens", lengths, lens)
    load("gt", cache_gates, gt)
    step = seqs // SPLIT

    def cache_copy(src, dst, sem, n):
        return pltpu.make_async_copy(
            src.at[pl.ds(n * step, step)], dst.at[pl.ds(n * step, step)], sem.at[n])

    k_loads = [cache_copy(cache_keys, kc, k_sem, n) for n in range(SPLIT)]
    v_loads = [cache_copy(cache_values, vc, v_sem, n) for n in range(SPLIT)]
    for copy in k_loads[:SPLIT // 2]:
        copy.start()

    phase("greet")
    barrier = pltpu.get_barrier_semaphore()

    for dz in range(nz):
        each(dz, lambda k: pl.semaphore_signal(
            barrier, inc=1, device_id=(peer(dz, k, True), core), device_id_type=MESH))
    pl.semaphore_signal(barrier, inc=1, device_id=(ep, 1 - core), device_id_type=MESH)

    phase("slots")
    ready("rt")
    for copy in k_loads[SPLIT // 2:]:
        copy.start()
    slot_id = iota((rows, 1), 0)
    magic = -(-4096 // CAP)
    assert all((l * magic) >> 12 == l // CAP for l in range(rows))
    peer_i = (slot_id * magic) >> 12
    rank_of = slot_id - peer_i * CAP
    lny, lnx, lb = log2(ny), log2(nx), log2(block)
    in_plane = peer_i & (block - 1)
    code = jnp.zeros_like(slot_id)
    for k in range(block):
        first, second = ((table[k][0] << lnx) + table[k][1] for table in tables)
        code = jnp.where(in_plane == k, by_core(first, second), code)
    dz, dy, dx = peer_i >> lb, code >> lnx, code & (nx - 1)
    expert_of = (
        (((z + dz) & (nz - 1)) << (lny + lnx)) + (((y + dy) & (ny - 1)) << lnx)
        + ((x + dx) & (nx - 1)))
    routed_to = rt[...]
    marks = jnp.zeros((rows, seqs), F32)
    marks_all = jnp.zeros((n_ep, seqs), F32)
    all_experts = iota((n_ep, seqs), 0)
    for k in range(top_k):
        marks = marks + (routed_to[k:k + 1, :] == expert_of).astype(F32)
        marks_all = marks_all + (routed_to[k:k + 1, :] == all_experts).astype(F32)
    earlier = (iota((seqs, seqs), 0) < iota((seqs, seqs), 1)).astype(F32)
    rank = dot(marks.astype(BF16), earlier.astype(BF16))
    pick = jnp.where(rank == rank_of.astype(F32), marks, 0.0)
    to_slot = (iota((rows, n_ep), 1) == expert_of).astype(F32)

    phase("project")
    ready("tok", "gain1", "wq")
    load("wk", w_key, wk)
    load("wv", w_value, wv)
    load("wf", w_forget, wf)
    for copy in v_loads[:SPLIT // 2]:
        copy.start()
    normed = norm_rows(tok[...].astype(F32), gain1[...].reshape(1, width))
    query = (dot(normed, wq[...]).astype(BF16).astype(F32)) * (HEAD_DIM ** -0.5)

    n_rows = 4 * seqs
    low = iota((seqs, 128), 1) < 64
    q0, q1 = query[:, :128], query[:, 128:]
    by_head = (
        jnp.where(low, q0, 0.0), jnp.where(low, pltpu.roll(q0, 64, 1), 0.0),
        jnp.where(low, 0.0, pltpu.roll(q1, 64, 1)), jnp.where(low, 0.0, q1),
    )
    for h in range(4):
        fanned[0, pl.ds(h, seqs, stride=4), :] = by_head[h]
    q_rows = fanned[0].astype(BF16)

    first = iota((8, 128), 0) < 4
    first_pos = iota((8, positions), 0) < 4
    pos = iota((8, positions), 1)
    for p in range(pairs):
        if p == 0:
            phase("k_wait0")
            ready("lens", "gt")
            for copy in k_loads[:SPLIT // 2]:
                copy.wait()
            for copy in v_loads[SPLIT // 2:]:
                copy.start()
            load("wo", w_out, wo)
            phase("score0")
        if p == pairs // 2:
            phase("k_wait1")
            for copy in k_loads[SPLIT // 2:]:
                copy.wait()
            phase("score1")
        q8 = q_rows[8 * p:8 * p + 8, :]
        zero = jnp.zeros_like(q8)
        q_pair = jnp.concatenate(
            [jnp.where(first, q8, zero), jnp.where(first, zero, q8)], axis=1)
        k_pair = jnp.concatenate([kc[2 * p], kc[2 * p + 1]], axis=1)
        s = dot(q_pair, k_pair, NT)
        g = jnp.concatenate([gt[2 * p], gt[2 * p + 1]], axis=0)
        count = jnp.where(first_pos, lens[2 * p], lens[2 * p + 1])
        last = jnp.sum(jnp.where(pos == count - 1, g, 0.0), axis=1, keepdims=True)
        s = s + (last - g)
        scores[8 * p:8 * p + 8, :] = jnp.where(pos < count, s, -jnp.inf)
    phase("project_kv")
    ready("wk", "wv", "wf")
    key_new = dot(normed, wk[...]).astype(BF16).astype(F32)
    value_new = dot(normed, wv[...]).astype(BF16).astype(F32)
    forget = dot(normed, wf[...], NT)
    forget = jnp.minimum(forget, 0.0) - jnp.log1p(jnp.exp(-jnp.abs(forget)))
    for h in range(4):
        of_head = pl.ds(h, seqs, stride=4)
        fanned[1, of_head, :] = key_new
        fanned[2, of_head, :] = value_new
        fanned[3, of_head, :] = jnp.broadcast_to(forget[:, h:h + 1], (seqs, 128))
    phase("softmax")
    self_score = jnp.sum(fanned[0] * fanned[1], axis=1, keepdims=True)
    s = scores[...] + fanned[3][:, :1]
    peak = jnp.maximum(jnp.max(s, axis=1, keepdims=True), self_score)
    weight = jnp.exp(s - peak)
    self_weight = jnp.exp(self_score - peak)
    total = jnp.sum(weight, axis=1, keepdims=True) + self_weight
    scores[...] = weight / total
    self_prob = (self_weight / total).astype(BF16).astype(F32)
    for p in range(pairs):
        if p == 0:
            phase("v_wait0")
            for copy in v_loads[:SPLIT // 2]:
                copy.wait()
            for item in later:
                load(*item)
            phase("values0")
        if p == pairs // 2:
            phase("v_wait1")
            for copy in v_loads[SPLIT // 2:]:
                copy.wait()
            ready("wo")
            phase("values1")
        prob = scores[8 * p:8 * p + 8, :].astype(BF16)
        v_pair = jnp.concatenate([vc[2 * p], vc[2 * p + 1]], axis=1)
        mixed = dot(prob, v_pair)
        heads[8 * p:8 * p + 8, :] = jnp.where(first, mixed[:, :128], mixed[:, 128:])
    heads[...] = heads[...] + self_prob * fanned[2]
    a0, a1, a2, a3 = (
        heads[pl.ds(h, seqs, stride=4), :].astype(BF16).astype(F32) for h in range(4))
    attn = jnp.concatenate([
        jnp.where(low, a0, pltpu.roll(a1, 64, 1)), jnp.where(low, pltpu.roll(a2, 64, 1), a3),
    ], axis=1).astype(BF16)
    mine[...] = dot(attn, wo[...]).astype(BF16)

    phase("barrier")
    pl.semaphore_wait(barrier, half + core)

    phase("swap_start")
    sibling = (ep, 1 - core)
    swap = pltpu.make_async_remote_copy(
        mine, theirs, att_sem.at[0], att_sem.at[1], device_id=sibling, device_id_type=MESH)
    swap.start()
    ready("gain2")
    phase("swap_wait")
    swap.wait_recv()
    phase("norm2")
    residual = (
        tok[...].astype(F32) + (mine[...].astype(F32) + theirs[...].astype(F32))).astype(BF16)
    kept[...] = residual
    keep = pltpu.make_async_copy(kept, out_residual, fin_sem.at[2])
    keep.start()
    ffn_rows = norm_rows(residual.astype(F32), gain2[...].reshape(1, width))

    phase("pack")

    def landed(dz, src, dst, send, recv, wait):
        def take(count):
            part = pl.ds(dz * block, count)
            wait(pltpu.make_async_remote_copy(
                src.at[part], dst.at[part], send.at[dz], recv.at[dz],
                device_id=sibling, device_id_type=MESH))

        here = jnp.logical_and(core == 0, dz == 0)
        pl.when(here)(lambda: take(block - 1) if block > 1 else None)
        pl.when(jnp.logical_not(here))(lambda: take(block))

    def go_landed(dz, wait):
        landed(dz, box_out, box_in, go_send, go_recv, wait)

    def back_landed(dz, wait):
        landed(dz, ret_out, ret_in, back_send, back_recv, wait)

    def go(dz, k):
        i = dz * block + k
        return pltpu.make_async_remote_copy(
            box_out.at[i], box_in.at[i], go_send.at[dz], go_recv.at[dz],
            device_id=(peer(dz, k, True), core), device_id_type=MESH)

    def back(dz, k):
        i = dz * block + k
        return pltpu.make_async_remote_copy(
            ret_out.at[i], ret_in.at[i], back_send.at[dz], back_recv.at[dz],
            device_id=(peer(dz, k, False), core), device_id_type=MESH)

    far_z = sorted(range(nz), key=lambda dz: -min(dz, nz - dz))
    lines = [pl.ds(j, b_rows, stride=cols) for j in range(cols)]
    box_shape = (block, CAP * cols, 128)

    for dz in far_z:
        chosen = pick[dz * b_rows:(dz + 1) * b_rows].astype(BF16)
        stage = lay.at[dz % z_step]
        for j in range(cols // 2):
            part = dot(chosen, ffn_rows[:, 256 * j:256 * j + 256])
            stage[lines[2 * j], :] = part[:, :128]
            stage[lines[2 * j + 1], :] = part[:, 128:]
        box_out[pl.ds(dz * block, block)] = stage[...].astype(BF16).reshape(box_shape)
        each(dz, lambda k: go(dz, k).start())

    @pl.when(core == 0)
    def _():
        box_in[block - 1] = box_out[block - 1]

    ready("eg", "eu", "ed")
    pushes = [
        pltpu.make_async_remote_copy(
            buf.at[0], buf.at[1], wt_send.at[n], wt_recv.at[n], device_id=sibling,
            device_id_type=MESH)
        for n, buf in enumerate((eg, eu, ed))
    ]
    for push in pushes:
        push.start()

    phase("shared")
    ready("rw")
    chance = dot(rw[...], ffn_rows, NT)
    chance = marks_all / (1.0 + jnp.exp(-chance))
    share = ROUTE_SCALE * chance / jnp.sum(chance, axis=0, keepdims=True)
    slot_w = dot(to_slot, share, precision=HIGH) * pick
    slot_hi = slot_w.astype(BF16).astype(F32)
    slot_w = jnp.concatenate([slot_hi, slot_w - slot_hi], axis=1)
    mix = [
        jnp.transpose(slot_w[dz * b_rows:(dz + 1) * b_rows]).astype(BF16) for dz in range(nz)
    ]
    ready("sg", "su", "sd")
    shared_h = (silu(dot(ffn_rows, sg[...])) * dot(ffn_rows, su[...])).astype(BF16)
    total_rows[...] = dot(shared_h, sd[...])

    hidden_w = eg.shape[2]
    phase("push_wait")
    for push in pushes:
        push.wait_recv()
    for first_z in range(0, nz, z_step):
        from_z = [(z + nz - first_z - n) % nz for n in range(z_step)]
        phase(f"go_wait{first_z}")
        for dz in from_z:
            go_landed(dz, lambda copy: copy.wait_recv())
        phase(f"unpack{first_z}")
        for n, dz in enumerate(from_z):
            lay[n] = box_in[pl.ds(dz * block, block)].reshape(b_rows * cols, 128).astype(F32)
        for j in range(cols):
            xs[:, 128 * j:128 * j + 128] = jnp.concatenate(
                [lay.at[n][lines[j], :] for n in range(z_step)], axis=0).astype(BF16)
        phase(f"ffn_in{first_z}")
        for part in range(2):
            gate = dot(xs[...], eg[part])
            up = dot(xs[...], eu[part])
            hid[:, hidden_w * part:hidden_w * (part + 1)] = (silu(gate) * up).astype(BF16)
        phase(f"ffn_out{first_z}")
        for j in range(cols // 2):
            down = ed[:, :, 256 * j:256 * j + 256].reshape(2 * hidden_w, 256)
            answer = dot(hid[...], down)
            for n in range(z_step):
                piece = answer[n * b_rows:(n + 1) * b_rows]
                lay.at[n][lines[2 * j], :] = piece[:, :128]
                lay.at[n][lines[2 * j + 1], :] = piece[:, 128:]
        for n, dz in enumerate(from_z):
            ret_out[pl.ds(dz * block, block)] = lay[n].astype(BF16).reshape(box_shape)
        phase(f"back_start{first_z}")
        for dz in from_z:
            each(dz, lambda k: back(dz, k).start())

    @pl.when(core == 0)
    def _():
        ret_in[block - 1] = ret_out[block - 1]

    near_z = far_z[::-1]
    for m in range(0, nz, z_step):
        phase(f"back_wait{m}")
        some = near_z[m:m + z_step]
        for dz in some:
            back_landed(dz, lambda copy: copy.wait_recv())
        phase(f"combine{m}")
        for n, dz in enumerate(some):
            lay[n] = ret_in[pl.ds(dz * block, block)].reshape(b_rows * cols, 128).astype(F32)
        for j in range(cols // 2):
            span = slice(256 * j, 256 * j + 256)
            part = total_rows[:, span]
            for n, dz in enumerate(some):
                answer = jnp.concatenate(
                    [lay.at[n][lines[2 * j], :], lay.at[n][lines[2 * j + 1], :]],
                    axis=1).astype(BF16)
                both = dot(mix[dz], answer)
                part = part + (both[:seqs] + both[seqs:])
            if m + z_step < nz:
                total_rows[:, span] = part
            else:
                fin_out[:, span] = part.astype(BF16)

    phase("finish")
    finish = pltpu.make_async_remote_copy(
        fin_out, out_theirs, fin_sem.at[0], fin_sem.at[1], device_id=sibling,
        device_id_type=MESH)
    finish.start()
    own = pltpu.make_async_copy(fin_out, out_mine, fin_sem.at[3])
    own.start()
    swap.wait_send()
    for push in pushes:
        push.wait_send()
    for dz in range(nz):
        go_landed(dz, lambda copy: copy.wait_send())
        back_landed(dz, lambda copy: copy.wait_send())
    keep.wait()
    own.wait()
    finish.wait_send()
    finish.wait_recv()
    phase()


def split_dims(n):
    return {64: (4, 4, 4), 4: (1, 2, 2), 8: (2, 2, 2)}[n]


def per_device(
    tokens, norm_gain, w_query, w_key, w_value, w_forget, w_out, cache_keys, cache_values,
    cache_gates, lengths, ffn_gain, router_w, routes, shared_gate, shared_up, shared_down,
    expert_gate, expert_up, expert_down,
):
    seqs, width = tokens.shape
    n_ep = lax.axis_size("ep")
    half = n_ep // 2
    dims = split_dims(n_ep)
    z_step = min(Z_STEP, dims[0])
    step_rows = half * CAP // dims[0] * z_step
    cols = width // 128
    positions = cache_keys.shape[1]
    ff = expert_gate.shape[2]
    any_spec = pl.BlockSpec(memory_space=pl.ANY)
    operands = (
        tokens, norm_gain, w_query, w_key, w_value, w_forget.T, w_out,
        cache_keys, cache_values, cache_gates, lengths, ffn_gain, router_w.T,
        routes.T, shared_gate, shared_up, shared_down, expert_gate, expert_up, expert_down,
    )
    vmem = pltpu.VMEM
    dma = pltpu.SemaphoreType.DMA

    def like(index):
        return vmem(operands[index].shape, operands[index].dtype)

    scratch = [
        like(0), like(1), like(2), like(3), like(4), like(5), like(6), like(7), like(8), like(9),
        pltpu.SMEM(lengths.shape, jnp.int32), like(11), like(12), like(13), like(14), like(15),
        like(16),
        vmem((2, width, ff), BF16), vmem((2, width, ff), BF16), vmem((2, ff, width), BF16),
        vmem((4 * seqs, positions), F32), vmem((4 * seqs, 128), F32),
        vmem((4, 4 * seqs, 128), F32),
        vmem((seqs, width), BF16), vmem((seqs, width), BF16), vmem((seqs, width), BF16),
        vmem((step_rows, width), BF16), vmem((step_rows, 2 * ff), BF16),
        vmem((z_step, step_rows // z_step * cols, 128), F32),
        vmem((half, CAP * cols, 128), BF16), vmem((half, CAP * cols, 128), BF16),
        vmem((half, CAP * cols, 128), BF16), vmem((half, CAP * cols, 128), BF16),
        vmem((seqs, width), F32), vmem((seqs, width), BF16),
        dma((SLOTS,)), dma((SPLIT,)), dma((SPLIT,)), dma((2,)), dma((3,)), dma((3,)),
        dma((dims[0],)), dma((dims[0],)), dma((dims[0],)), dma((dims[0],)), dma((4,)),
    ]
    residual, own, other = pl.pallas_call(
        functools.partial(kernel, dims),
        out_shape=[jax.ShapeDtypeStruct((seqs, width), BF16)] * 3,
        in_specs=[any_spec] * len(operands),
        out_specs=[any_spec] * 3,
        scratch_shapes=scratch,
        compiler_params=pltpu.CompilerParams(
            collective_id=0, has_side_effects=True, vmem_limit_bytes=62 * 1024 * 1024),
    )(*operands)
    return (residual.astype(F32) + (own.astype(F32) + other.astype(F32))).astype(BF16)


def solution(mesh):
    placed = (
        P("ep", None),
        P(),
        P(None, "tp"),
        P(None, "tp"),
        P(None, "tp"),
        P(None, "tp"),
        P("tp", None),
        P("ep", None, "tp"),
        P("ep", None, "tp"),
        P("ep", "tp", None),
        P("ep"),
        P(),
        P(),
        P("ep", None),
        P(None, "tp"),
        P(None, "tp"),
        P("tp", None),
        P("ep", None, "tp"),
        P("ep", None, "tp"),
        P("ep", "tp", None),
    )
    return jax.shard_map(
        per_device, mesh=mesh, in_specs=placed, out_specs=P("ep", None), check_vma=False
    )
```

```python
import functools

import jax
import jax.numpy as jnp
from jax import lax
from jax.experimental import pallas as pl
from jax.experimental.pallas import tpu as pltpu
from jax.sharding import PartitionSpec as P

HEAD_DIM = 64
EPS = 1e-06
ROUTE_SCALE = 2.5
CAP = 3
Z_STEP = 2
SLOTS = 9
PIECES = 2
MESH = pl.DeviceIdType.MESH
F32 = jnp.float32
BF16 = jnp.bfloat16
HIGH = lax.Precision.HIGHEST
NT = (((1,), (1,)), ((), ()))
TN = (((0,), (0,)), ((), ()))
NN = (((1,), (0,)), ((), ()))


def dot(left, right, dims=NN, precision=None):
    return lax.dot_general(left, right, dims, precision=precision, preferred_element_type=F32)


def iota(shape, dim):
    return lax.broadcasted_iota(jnp.int32, shape, dim)


def norm_rows(values, gain):
    factor = lax.rsqrt(jnp.mean(values * values, axis=-1, keepdims=True) + EPS)
    return (values * factor * gain.astype(F32)).astype(BF16)


def silu(x):
    return x / (1.0 + jnp.exp(-x))


class Phases:
    def __init__(self):
        self.scope = None

    def __call__(self, name=None):
        if self.scope is not None:
            self.scope.__exit__(None, None, None)
        self.scope = jax.named_scope(name) if name else None
        if self.scope is not None:
            self.scope.__enter__()


def plane_tables(dims):
    ny, nx = dims[1:]

    def far(entry):
        return min(entry[0], ny - entry[0]) + min(entry[1], nx - entry[1])

    entries = [(dy, dx) for dy in range(ny) for dx in range(nx)]
    entries.sort(key=lambda entry: (-far(entry), entry))
    half = len(entries) // 2
    pairs, single = [], []
    for entry in entries:
        other = ((ny - entry[0]) % ny, (nx - entry[1]) % nx)
        if other == entry:
            single.append(entry)
        elif entry < other:
            pairs.append([entry, other])
    cut = len(pairs) // 2
    second = sum(pairs[:cut], [])
    fill = half - len(second)
    tables = (sum(pairs[cut:], []) + single[fill:], second + single[:fill])
    for table in tables:
        table.sort(key=lambda entry: -far(entry))
    assert len(tables[0]) == len(tables[1])
    return tables


def log2(n):
    assert n & (n - 1) == 0
    return n.bit_length() - 1


def kernel(
    dims,
    tokens, norm_gain, w_query, w_key, w_value, w_forget, w_out, cache_keys, cache_values,
    cache_gates, lengths, ffn_gain, router_w, routes, shared_gate, shared_up, shared_down,
    expert_gate, expert_up, expert_down,
    out_residual, out_mine, out_theirs,
    tok, gain1, wq, wk, wv, wf, wo, kc, vc, gt, lens, gain2, rw, rt, sg, su, sd,
    eg, eu, ed, scores, heads, fanned, mine, theirs, xs, hid, lay, box_out, box_in, ret_out, ret_in,
    total_rows,
    in_sem, k_sem, v_sem, att_sem, wt_send, wt_recv, go_send, go_recv, back_send, back_recv,
    fin_sem,
):
    nz, ny, nx = dims
    n_ep = nz * ny * nx
    half = n_ep // 2
    block = half // nz
    seqs, width = tokens.shape
    positions = cache_keys.shape[1]
    top_k = routes.shape[0]
    cols = width // 128
    rows = half * CAP
    b_rows = block * CAP
    z_step = min(Z_STEP, nz)
    pairs = seqs // 2
    ep = lax.axis_index("ep")
    core = lax.axis_index("tp")
    z, y, x = ep // (ny * nx), (ep // nx) % ny, ep % nx
    tables = plane_tables(dims)

    def by_core(first, second):
        return first if first == second else first + core * (second - first)

    def peer(dz, k, forward):
        dy, dx = (by_core(a, b) for a, b in zip(tables[0][k], tables[1][k]))
        if forward:
            pz, py, px = (z + dz) % nz, (y + dy) % ny, (x + dx) % nx
        else:
            pz, py, px = (z + nz - dz) % nz, (y + ny - dy) % ny, (x + nx - dx) % nx
        return (pz * ny + py) * nx + px

    def each(dz, action):
        for k in range(block - 1):
            action(k)
        here = jnp.logical_and(core == 0, dz == 0)
        pl.when(jnp.logical_not(here))(functools.partial(action, block - 1))

    phase = Phases()
    phase("loads")
    loads = {}
    order = (
        ("rt", routes, rt), ("tok", tokens, tok), ("gain1", norm_gain, gain1),
    )
    later = (
        ("rw", router_w, rw), ("gain2", ffn_gain, gain2),
        ("eg", expert_gate.at[0], eg.at[0]), ("eu", expert_up.at[0], eu.at[0]),
        ("ed", expert_down.at[0], ed.at[0]),
        ("sg", shared_gate, sg), ("su", shared_up, su), ("sd", shared_down, sd),
    )
    slot = 0

    def load(name, src, dst, pieces=1):
        nonlocal slot
        sem = in_sem.at[slot % SLOTS]
        loads[name] = pltpu.make_async_copy(src, dst, sem)
        size = src.shape[0] // pieces
        for n in range(pieces):
            part = pl.ds(n * size, size)
            if pieces == 1:
                loads[name].start()
            else:
                pltpu.make_async_copy(src.at[part], dst.at[part], sem).start()
        slot += 1

    def ready(*names):
        for name in names:
            loads[name].wait()

    for item in order:
        load(*item)
    load("wq", w_query, wq, 4)
    load("lens", lengths, lens)
    load("gt", cache_gates, gt)
    step = seqs // (2 * PIECES)

    def cache_half(src, dst, sem, n):
        for piece in range(PIECES):
            part = pl.ds((n * PIECES + piece) * step, step)
            pltpu.make_async_copy(src.at[part], dst.at[part], sem.at[n]).start()
        part = pl.ds(n * PIECES * step, PIECES * step)
        return pltpu.make_async_copy(src.at[part], dst.at[part], sem.at[n])

    k_half = [cache_half(cache_keys, kc, k_sem, 0)]
    v_half = []

    phase("greet")
    barrier = pltpu.get_barrier_semaphore()

    far_z = sorted(range(nz), key=lambda dz: -min(dz, nz - dz))
    for dz in far_z:
        each(dz, lambda k: pl.semaphore_signal(
            barrier, inc=1, device_id=(peer(dz, k, True), core), device_id_type=MESH))
    pl.semaphore_signal(barrier, inc=1, device_id=(ep, 1 - core), device_id_type=MESH)

    phase("slots")
    ready("rt")
    k_half.append(cache_half(cache_keys, kc, k_sem, 1))
    slot_id = iota((rows, 1), 0)
    magic = -(-4096 // CAP)
    assert all((l * magic) >> 12 == l // CAP for l in range(rows))
    peer_i = (slot_id * magic) >> 12
    rank_of = slot_id - peer_i * CAP
    lny, lnx, lb = log2(ny), log2(nx), log2(block)
    in_plane = peer_i & (block - 1)
    code = jnp.zeros_like(slot_id)
    for k in range(block):
        first, second = ((table[k][0] << lnx) + table[k][1] for table in tables)
        code = jnp.where(in_plane == k, by_core(first, second), code)
    dz, dy, dx = peer_i >> lb, code >> lnx, code & (nx - 1)
    expert_of = (
        (((z + dz) & (nz - 1)) << (lny + lnx)) + (((y + dy) & (ny - 1)) << lnx)
        + ((x + dx) & (nx - 1)))
    routed_to = rt[...]
    marks = jnp.zeros((rows, seqs), F32)
    marks_all = jnp.zeros((n_ep, seqs), F32)
    all_experts = iota((n_ep, seqs), 0)
    for k in range(top_k):
        marks = marks + (routed_to[k:k + 1, :] == expert_of).astype(F32)
        marks_all = marks_all + (routed_to[k:k + 1, :] == all_experts).astype(F32)
    earlier = (iota((seqs, seqs), 0) < iota((seqs, seqs), 1)).astype(F32)
    rank = dot(marks.astype(BF16), earlier.astype(BF16))
    pick = jnp.where(rank == rank_of.astype(F32), marks, 0.0)
    to_slot = (iota((rows, n_ep), 1) == expert_of).astype(F32)

    phase("project")
    ready("tok", "gain1", "wq")
    load("wk", w_key, wk)
    load("wv", w_value, wv)
    load("wf", w_forget, wf)
    v_half.append(cache_half(cache_values, vc, v_sem, 0))
    normed = norm_rows(tok[...].astype(F32), gain1[...].reshape(1, width))
    query = (dot(normed, wq[...]).astype(BF16).astype(F32)) * (HEAD_DIM ** -0.5)

    n_rows = 4 * seqs
    low = iota((seqs, 128), 1) < 64
    q0, q1 = query[:, :128], query[:, 128:]
    by_head = (
        jnp.where(low, q0, 0.0), jnp.where(low, pltpu.roll(q0, 64, 1), 0.0),
        jnp.where(low, 0.0, pltpu.roll(q1, 64, 1)), jnp.where(low, 0.0, q1),
    )
    for h in range(4):
        fanned[0, pl.ds(h, seqs, stride=4), :] = by_head[h]
    q_rows = fanned[0].astype(BF16)

    first = iota((8, 128), 0) < 4
    first_pos = iota((8, positions), 0) < 4
    pos = iota((8, positions), 1)
    for p in range(pairs):
        if p == 0:
            phase("k_wait0")
            ready("lens", "gt")
            k_half[0].wait()
            v_half.append(cache_half(cache_values, vc, v_sem, 1))
            load("wo", w_out, wo)
            phase("score0")
        if p == pairs // 2:
            phase("k_wait1")
            k_half[1].wait()
            phase("score1")
        q8 = q_rows[8 * p:8 * p + 8, :]
        zero = jnp.zeros_like(q8)
        q_pair = jnp.concatenate(
            [jnp.where(first, q8, zero), jnp.where(first, zero, q8)], axis=1)
        k_pair = jnp.concatenate([kc[2 * p], kc[2 * p + 1]], axis=1)
        s = dot(q_pair, k_pair, NT)
        g = jnp.concatenate([gt[2 * p], gt[2 * p + 1]], axis=0)
        count = jnp.where(first_pos, lens[2 * p], lens[2 * p + 1])
        last = jnp.sum(jnp.where(pos == count - 1, g, 0.0), axis=1, keepdims=True)
        s = s + (last - g)
        scores[8 * p:8 * p + 8, :] = jnp.where(pos < count, s, -jnp.inf)
    phase("project_kv")
    ready("wk", "wv", "wf")
    key_new = dot(normed, wk[...]).astype(BF16).astype(F32)
    value_new = dot(normed, wv[...]).astype(BF16).astype(F32)
    forget = dot(normed, wf[...], NT)
    forget = jnp.minimum(forget, 0.0) - jnp.log1p(jnp.exp(-jnp.abs(forget)))
    for h in range(4):
        of_head = pl.ds(h, seqs, stride=4)
        fanned[1, of_head, :] = key_new
        fanned[2, of_head, :] = value_new
        fanned[3, of_head, :] = jnp.broadcast_to(forget[:, h:h + 1], (seqs, 128))
    phase("softmax")
    self_score = jnp.sum(fanned[0] * fanned[1], axis=1, keepdims=True)
    s = scores[...] + fanned[3][:, :1]
    peak = jnp.maximum(jnp.max(s, axis=1, keepdims=True), self_score)
    weight = jnp.exp(s - peak)
    self_weight = jnp.exp(self_score - peak)
    total = jnp.sum(weight, axis=1, keepdims=True) + self_weight
    scores[...] = weight / total
    self_prob = (self_weight / total).astype(BF16).astype(F32)
    for p in range(pairs):
        if p == 0:
            phase("v_wait0")
            v_half[0].wait()
            for item in later:
                load(*item)
            phase("values0")
        if p == pairs // 2:
            phase("v_wait1")
            v_half[1].wait()
            ready("wo")
            phase("values1")
        prob = scores[8 * p:8 * p + 8, :].astype(BF16)
        v_pair = jnp.concatenate([vc[2 * p], vc[2 * p + 1]], axis=1)
        mixed = dot(prob, v_pair)
        heads[8 * p:8 * p + 8, :] = jnp.where(first, mixed[:, :128], mixed[:, 128:])
    heads[...] = heads[...] + self_prob * fanned[2]
    a0, a1, a2, a3 = (
        heads[pl.ds(h, seqs, stride=4), :].astype(BF16).astype(F32) for h in range(4))
    attn = jnp.concatenate([
        jnp.where(low, a0, pltpu.roll(a1, 64, 1)), jnp.where(low, pltpu.roll(a2, 64, 1), a3),
    ], axis=1).astype(BF16)
    mine[...] = dot(attn, wo[...]).astype(BF16)

    phase("barrier")
    pl.semaphore_wait(barrier, half + core)

    phase("swap_start")
    sibling = (ep, 1 - core)
    swap = pltpu.make_async_remote_copy(
        mine, theirs, att_sem.at[0], att_sem.at[1], device_id=sibling, device_id_type=MESH)
    swap.start()
    ready("gain2")
    phase("swap_wait")
    swap.wait_recv()
    phase("norm2")
    residual = (
        tok[...].astype(F32) + (mine[...].astype(F32) + theirs[...].astype(F32))).astype(BF16)
    out_residual[...] = residual
    ffn_rows = norm_rows(residual.astype(F32), gain2[...].reshape(1, width))

    phase("pack")

    def landed(dz, src, dst, send, recv):
        def take(count):
            part = pl.ds(dz * block, count)
            pltpu.make_async_remote_copy(
                src.at[part], dst.at[part], send.at[0], recv.at[dz],
                device_id=sibling, device_id_type=MESH).wait_recv()

        here = jnp.logical_and(core == 0, dz == 0)
        pl.when(here)(lambda: take(block - 1) if block > 1 else None)
        pl.when(jnp.logical_not(here))(lambda: take(block))

    def go_landed(dz):
        landed(dz, box_out, box_in, go_send, go_recv)

    def back_landed(dz):
        landed(dz, ret_out, ret_in, back_send, back_recv)

    def sent(src, dst, send, recv):
        def take(count):
            part = pl.ds(0, count)
            pltpu.make_async_remote_copy(
                src.at[part], dst.at[part], send.at[0], recv.at[0],
                device_id=sibling, device_id_type=MESH).wait_send()

        pl.when(core == 0)(lambda: take(half - 1))
        pl.when(core == 1)(lambda: take(half))

    def go(dz, k):
        i = dz * block + k
        return pltpu.make_async_remote_copy(
            box_out.at[i], box_in.at[i], go_send.at[0], go_recv.at[dz],
            device_id=(peer(dz, k, True), core), device_id_type=MESH)

    def back(dz, k):
        i = dz * block + k
        return pltpu.make_async_remote_copy(
            ret_out.at[i], ret_in.at[i], back_send.at[0], back_recv.at[dz],
            device_id=(peer(dz, k, False), core), device_id_type=MESH)

    lines = [pl.ds(j, b_rows, stride=cols) for j in range(cols)]
    box_shape = (block, CAP * cols, 128)

    for dz in far_z:
        chosen = pick[dz * b_rows:(dz + 1) * b_rows].astype(BF16)
        stage = lay.at[dz % z_step]
        for j in range(cols // 2):
            part = dot(chosen, ffn_rows[:, 256 * j:256 * j + 256])
            stage[lines[2 * j], :] = part[:, :128]
            stage[lines[2 * j + 1], :] = part[:, 128:]
        box_out[pl.ds(dz * block, block)] = stage[...].astype(BF16).reshape(box_shape)
        each(dz, lambda k: go(dz, k).start())

    @pl.when(core == 0)
    def _():
        box_in[block - 1] = box_out[block - 1]

    ready("eg", "eu", "ed")
    pushes = [
        pltpu.make_async_remote_copy(
            buf.at[0], buf.at[1], wt_send.at[n], wt_recv.at[n], device_id=sibling,
            device_id_type=MESH)
        for n, buf in enumerate((eg, eu, ed))
    ]
    for push in pushes:
        push.start()

    phase("shared")
    ready("rw")
    chance = dot(rw[...], ffn_rows, NT)
    chance = marks_all / (1.0 + jnp.exp(-chance))
    share = ROUTE_SCALE * chance / jnp.sum(chance, axis=0, keepdims=True)
    slot_w = dot(to_slot, share, precision=HIGH) * pick
    slot_hi = slot_w.astype(BF16).astype(F32)
    slot_w = jnp.concatenate([slot_hi, slot_w - slot_hi], axis=1)
    mix = [
        jnp.transpose(slot_w[dz * b_rows:(dz + 1) * b_rows]).astype(BF16) for dz in range(nz)
    ]
    ready("sg", "su", "sd")
    shared_h = (silu(dot(ffn_rows, sg[...])) * dot(ffn_rows, su[...])).astype(BF16)
    total_rows[...] = dot(shared_h, sd[...])

    hidden_w = eg.shape[2]
    phase("push_wait")
    for push in pushes:
        push.wait_recv()
    for first_z in range(0, nz, z_step):
        from_z = [(z + nz - first_z - n) % nz for n in range(z_step)]
        phase(f"go_wait{first_z}")
        for dz in from_z:
            go_landed(dz)
        phase(f"unpack{first_z}")
        for n, dz in enumerate(from_z):
            lay[n] = box_in[pl.ds(dz * block, block)].reshape(b_rows * cols, 128).astype(F32)
        for j in range(cols):
            xs[:, 128 * j:128 * j + 128] = jnp.concatenate(
                [lay.at[n][lines[j], :] for n in range(z_step)], axis=0).astype(BF16)
        phase(f"ffn_in{first_z}")
        for part in range(2):
            gate = dot(xs[...], eg[part])
            up = dot(xs[...], eu[part])
            hid[:, hidden_w * part:hidden_w * (part + 1)] = (silu(gate) * up).astype(BF16)
        phase(f"ffn_out{first_z}")
        for j in range(cols // 2):
            down = ed[:, :, 256 * j:256 * j + 256].reshape(2 * hidden_w, 256)
            answer = dot(hid[...], down)
            for n in range(z_step):
                piece = answer[n * b_rows:(n + 1) * b_rows]
                lay.at[n][lines[2 * j], :] = piece[:, :128]
                lay.at[n][lines[2 * j + 1], :] = piece[:, 128:]
        for n, dz in enumerate(from_z):
            ret_out[pl.ds(dz * block, block)] = lay[n].astype(BF16).reshape(box_shape)
        phase(f"back_start{first_z}")
        for dz in from_z:
            each(dz, lambda k: back(dz, k).start())

    @pl.when(core == 0)
    def _():
        ret_in[block - 1] = ret_out[block - 1]

    near_z = far_z[::-1]
    lots = [near_z[:z_step]] + [[dz] for dz in near_z[z_step:]]
    for m, some in enumerate(lots):
        phase(f"back_wait{m}")
        for dz in some:
            back_landed(dz)
        phase(f"combine{m}")
        for n, dz in enumerate(some):
            lay[n] = ret_in[pl.ds(dz * block, block)].reshape(b_rows * cols, 128).astype(F32)
        for j in range(cols // 2):
            span = slice(256 * j, 256 * j + 256)
            part = total_rows[:, span]
            for n, dz in enumerate(some):
                answer = jnp.concatenate(
                    [lay.at[n][lines[2 * j], :], lay.at[n][lines[2 * j + 1], :]],
                    axis=1).astype(BF16)
                both = dot(mix[dz], answer)
                part = part + (both[:seqs] + both[seqs:])
            if m + 1 < len(lots):
                total_rows[:, span] = part
            else:
                out_mine[:, span] = part.astype(BF16)

    phase("finish")
    finish = pltpu.make_async_remote_copy(
        out_mine, out_theirs, fin_sem.at[0], fin_sem.at[1], device_id=sibling,
        device_id_type=MESH)
    finish.start()
    swap.wait_send()
    for push in pushes:
        push.wait_send()
    sent(box_out, box_in, go_send, go_recv)
    sent(ret_out, ret_in, back_send, back_recv)
    finish.wait_send()
    finish.wait_recv()
    phase()


def split_dims(n):
    return {64: (4, 4, 4), 4: (1, 2, 2), 8: (2, 2, 2)}[n]


def per_device(
    tokens, norm_gain, w_query, w_key, w_value, w_forget, w_out, cache_keys, cache_values,
    cache_gates, lengths, ffn_gain, router_w, routes, shared_gate, shared_up, shared_down,
    expert_gate, expert_up, expert_down,
):
    seqs, width = tokens.shape
    n_ep = lax.axis_size("ep")
    half = n_ep // 2
    dims = split_dims(n_ep)
    z_step = min(Z_STEP, dims[0])
    step_rows = half * CAP // dims[0] * z_step
    cols = width // 128
    positions = cache_keys.shape[1]
    ff = expert_gate.shape[2]
    any_spec = pl.BlockSpec(memory_space=pl.ANY)
    operands = (
        tokens, norm_gain, w_query, w_key, w_value, w_forget.T, w_out,
        cache_keys, cache_values, cache_gates, lengths, ffn_gain, router_w.T,
        routes.T, shared_gate, shared_up, shared_down, expert_gate, expert_up, expert_down,
    )
    operands = tuple(
        pltpu.with_memory_space_constraint(operand, pltpu.HBM) for operand in operands)
    vmem = pltpu.VMEM
    dma = pltpu.SemaphoreType.DMA

    def like(index):
        return vmem(operands[index].shape, operands[index].dtype)

    scratch = [
        like(0), like(1), like(2), like(3), like(4), like(5), like(6), like(7), like(8), like(9),
        pltpu.SMEM(lengths.shape, jnp.int32), like(11), like(12), like(13), like(14), like(15),
        like(16),
        vmem((2, width, ff), BF16), vmem((2, width, ff), BF16), vmem((2, ff, width), BF16),
        vmem((4 * seqs, positions), F32), vmem((4 * seqs, 128), F32),
        vmem((4, 4 * seqs, 128), F32),
        vmem((seqs, width), BF16), vmem((seqs, width), BF16),
        vmem((step_rows, width), BF16), vmem((step_rows, 2 * ff), BF16),
        vmem((z_step, step_rows // z_step * cols, 128), F32),
        vmem((half, CAP * cols, 128), BF16), vmem((half, CAP * cols, 128), BF16),
        vmem((half, CAP * cols, 128), BF16), vmem((half, CAP * cols, 128), BF16),
        vmem((seqs, width), F32),
        dma((SLOTS,)), dma((2,)), dma((2,)), dma((2,)), dma((3,)), dma((3,)),
        dma((1,)), dma((dims[0],)), dma((1,)), dma((dims[0],)), dma((2,)),
    ]
    residual, own, other = pl.pallas_call(
        functools.partial(kernel, dims),
        out_shape=[jax.ShapeDtypeStruct((seqs, width), BF16)] * 3,
        in_specs=[any_spec] * len(operands),
        out_specs=[pl.BlockSpec(memory_space=pltpu.VMEM)] * 3,
        scratch_shapes=scratch,
        compiler_params=pltpu.CompilerParams(
            collective_id=0, has_side_effects=True, vmem_limit_bytes=32 * 1024 * 1024),
    )(*operands)
    return (residual.astype(F32) + (own.astype(F32) + other.astype(F32))).astype(BF16)


def solution(mesh):
    placed = (
        P("ep", None),
        P(),
        P(None, "tp"),
        P(None, "tp"),
        P(None, "tp"),
        P(None, "tp"),
        P("tp", None),
        P("ep", None, "tp"),
        P("ep", None, "tp"),
        P("ep", "tp", None),
        P("ep"),
        P(),
        P(),
        P("ep", None),
        P(None, "tp"),
        P(None, "tp"),
        P("tp", None),
        P("ep", None, "tp"),
        P("ep", None, "tp"),
        P("ep", "tp", None),
    )
    return jax.shard_map(
        per_device, mesh=mesh, in_specs=placed, out_specs=P("ep", None), check_vma=False
    )
```

```python
import functools

import jax
import jax.numpy as jnp
from jax import lax
from jax.experimental import pallas as pl
from jax.experimental.pallas import tpu as pltpu
from jax.sharding import PartitionSpec as P

HEAD_DIM = 64
EPS = 1e-06
ROUTE_SCALE = 2.5
CAP = 3
Z_STEP = 3
SLOTS = 9
PIECES = 2
MESH = pl.DeviceIdType.MESH
F32 = jnp.float32
BF16 = jnp.bfloat16
HIGH = lax.Precision.HIGHEST
NT = (((1,), (1,)), ((), ()))
TN = (((0,), (0,)), ((), ()))
NN = (((1,), (0,)), ((), ()))


def dot(left, right, dims=NN, precision=None):
    return lax.dot_general(left, right, dims, precision=precision, preferred_element_type=F32)


def iota(shape, dim):
    return lax.broadcasted_iota(jnp.int32, shape, dim)


def norm_rows(values, gain):
    factor = lax.rsqrt(jnp.mean(values * values, axis=-1, keepdims=True) + EPS)
    return (values * factor * gain.astype(F32)).astype(BF16)


def silu(x):
    return x / (1.0 + jnp.exp(-x))


class Phases:
    def __init__(self):
        self.scope = None

    def __call__(self, name=None):
        if self.scope is not None:
            self.scope.__exit__(None, None, None)
        self.scope = jax.named_scope(name) if name else None
        if self.scope is not None:
            self.scope.__enter__()


def plane_tables(dims):
    ny, nx = dims[1:]

    def far(entry):
        return min(entry[0], ny - entry[0]) + min(entry[1], nx - entry[1])

    entries = [(dy, dx) for dy in range(ny) for dx in range(nx)]
    entries.sort(key=lambda entry: (-far(entry), entry))
    half = len(entries) // 2
    pairs, single = [], []
    for entry in entries:
        other = ((ny - entry[0]) % ny, (nx - entry[1]) % nx)
        if other == entry:
            single.append(entry)
        elif entry < other:
            pairs.append([entry, other])
    cut = len(pairs) // 2
    second = sum(pairs[:cut], [])
    fill = half - len(second)
    tables = (sum(pairs[cut:], []) + single[fill:], second + single[:fill])
    for table in tables:
        table.sort(key=lambda entry: -far(entry))
    assert len(tables[0]) == len(tables[1])
    return tables


def log2(n):
    assert n & (n - 1) == 0
    return n.bit_length() - 1


def kernel(
    dims,
    tokens, norm_gain, w_query, w_key, w_value, w_forget, w_out, cache_keys, cache_values,
    cache_gates, lengths, ffn_gain, router_w, routes, shared_gate, shared_up, shared_down,
    expert_gate, expert_up, expert_down,
    out_residual, out_mine, out_theirs,
    tok, gain1, wq, wk, wv, wf, wo, kc, vc, gt, lens, gain2, rw, rt, sg, su, sd,
    eg, eu, ed, scores, heads, fanned, mine, theirs, xs, hid, lay, box_out, box_in, ret_out, ret_in,
    total_rows,
    in_sem, k_sem, v_sem, att_sem, wt_send, wt_recv, go_send, go_recv, back_send, back_recv,
    fin_sem,
):
    nz, ny, nx = dims
    n_ep = nz * ny * nx
    half = n_ep // 2
    block = half // nz
    seqs, width = tokens.shape
    positions = cache_keys.shape[1]
    top_k = routes.shape[0]
    cols = width // 128
    rows = half * CAP
    b_rows = block * CAP
    z_step = min(Z_STEP, nz)
    pairs = seqs // 2
    ep = lax.axis_index("ep")
    core = lax.axis_index("tp")
    z, y, x = ep // (ny * nx), (ep // nx) % ny, ep % nx
    tables = plane_tables(dims)

    def by_core(first, second):
        return first if first == second else first + core * (second - first)

    def peer(dz, k, forward):
        dy, dx = (by_core(a, b) for a, b in zip(tables[0][k], tables[1][k]))
        if forward:
            pz, py, px = (z + dz) % nz, (y + dy) % ny, (x + dx) % nx
        else:
            pz, py, px = (z + nz - dz) % nz, (y + ny - dy) % ny, (x + nx - dx) % nx
        return (pz * ny + py) * nx + px

    def each(dz, action):
        for k in range(block - 1):
            action(k)
        here = jnp.logical_and(core == 0, dz == 0)
        pl.when(jnp.logical_not(here))(functools.partial(action, block - 1))

    phase = Phases()
    phase("loads")
    loads = {}
    order = (
        ("rt", routes, rt), ("tok", tokens, tok), ("gain1", norm_gain, gain1),
    )
    later = (
        ("rw", router_w, rw), ("gain2", ffn_gain, gain2),
        ("eg", expert_gate.at[0], eg.at[0]), ("eu", expert_up.at[0], eu.at[0]),
        ("ed", expert_down.at[0], ed.at[0]),
        ("sg", shared_gate, sg), ("su", shared_up, su), ("sd", shared_down, sd),
    )
    slot = 0

    def load(name, src, dst, pieces=1):
        nonlocal slot
        sem = in_sem.at[slot % SLOTS]
        loads[name] = pltpu.make_async_copy(src, dst, sem)
        size = src.shape[0] // pieces
        for n in range(pieces):
            part = pl.ds(n * size, size)
            if pieces == 1:
                loads[name].start()
            else:
                pltpu.make_async_copy(src.at[part], dst.at[part], sem).start()
        slot += 1

    def ready(*names):
        for name in names:
            loads[name].wait()

    for item in order:
        load(*item)
    load("wq", w_query, wq, 4)
    load("lens", lengths, lens)
    load("gt", cache_gates, gt)
    step = seqs // (2 * PIECES)

    def cache_half(src, dst, sem, n):
        for piece in range(PIECES):
            part = pl.ds((n * PIECES + piece) * step, step)
            pltpu.make_async_copy(src.at[part], dst.at[part], sem.at[n]).start()
        part = pl.ds(n * PIECES * step, PIECES * step)
        return pltpu.make_async_copy(src.at[part], dst.at[part], sem.at[n])

    k_half = [cache_half(cache_keys, kc, k_sem, 0)]
    v_half = []

    phase("greet")
    barrier = pltpu.get_barrier_semaphore()

    far_z = sorted(range(nz), key=lambda dz: -min(dz, nz - dz))
    for dz in far_z:
        each(dz, lambda k: pl.semaphore_signal(
            barrier, inc=1, device_id=(peer(dz, k, True), core), device_id_type=MESH))
    pl.semaphore_signal(barrier, inc=1, device_id=(ep, 1 - core), device_id_type=MESH)

    phase("slots")
    ready("rt")
    k_half.append(cache_half(cache_keys, kc, k_sem, 1))
    slot_id = iota((rows, 1), 0)
    magic = -(-4096 // CAP)
    assert all((l * magic) >> 12 == l // CAP for l in range(rows))
    peer_i = (slot_id * magic) >> 12
    rank_of = slot_id - peer_i * CAP
    lny, lnx, lb = log2(ny), log2(nx), log2(block)
    in_plane = peer_i & (block - 1)
    code = jnp.zeros_like(slot_id)
    for k in range(block):
        first, second = ((table[k][0] << lnx) + table[k][1] for table in tables)
        code = jnp.where(in_plane == k, by_core(first, second), code)
    dz, dy, dx = peer_i >> lb, code >> lnx, code & (nx - 1)
    expert_of = (
        (((z + dz) & (nz - 1)) << (lny + lnx)) + (((y + dy) & (ny - 1)) << lnx)
        + ((x + dx) & (nx - 1)))
    routed_to = rt[...]
    marks = jnp.zeros((rows, seqs), F32)
    marks_all = jnp.zeros((n_ep, seqs), F32)
    all_experts = iota((n_ep, seqs), 0)
    for k in range(top_k):
        marks = marks + (routed_to[k:k + 1, :] == expert_of).astype(F32)
        marks_all = marks_all + (routed_to[k:k + 1, :] == all_experts).astype(F32)
    earlier = (iota((seqs, seqs), 0) < iota((seqs, seqs), 1)).astype(F32)
    rank = dot(marks.astype(BF16), earlier.astype(BF16))
    pick = jnp.where(rank == rank_of.astype(F32), marks, 0.0)
    to_slot = (iota((rows, n_ep), 1) == expert_of).astype(F32)

    phase("project")
    ready("tok", "gain1", "wq")
    load("wk", w_key, wk)
    load("wv", w_value, wv)
    load("wf", w_forget, wf)
    v_half.append(cache_half(cache_values, vc, v_sem, 0))
    normed = norm_rows(tok[...].astype(F32), gain1[...].reshape(1, width))
    query = (dot(normed, wq[...]).astype(BF16).astype(F32)) * (HEAD_DIM ** -0.5)

    n_rows = 4 * seqs
    low = iota((seqs, 128), 1) < 64
    q0, q1 = query[:, :128], query[:, 128:]
    by_head = (
        jnp.where(low, q0, 0.0), jnp.where(low, pltpu.roll(q0, 64, 1), 0.0),
        jnp.where(low, 0.0, pltpu.roll(q1, 64, 1)), jnp.where(low, 0.0, q1),
    )
    for h in range(4):
        fanned[0, pl.ds(h, seqs, stride=4), :] = by_head[h]
    q_rows = fanned[0].astype(BF16)

    first = iota((8, 128), 0) < 4
    first_pos = iota((8, positions), 0) < 4
    pos = iota((8, positions), 1)
    for p in range(pairs):
        if p == 0:
            phase("k_wait0")
            ready("lens", "gt")
            k_half[0].wait()
            v_half.append(cache_half(cache_values, vc, v_sem, 1))
            load("wo", w_out, wo)
            phase("score0")
        if p == pairs // 2:
            phase("k_wait1")
            k_half[1].wait()
            phase("score1")
        q8 = q_rows[8 * p:8 * p + 8, :]
        zero = jnp.zeros_like(q8)
        q_pair = jnp.concatenate(
            [jnp.where(first, q8, zero), jnp.where(first, zero, q8)], axis=1)
        k_pair = jnp.concatenate([kc[2 * p], kc[2 * p + 1]], axis=1)
        s = dot(q_pair, k_pair, NT)
        g = jnp.concatenate([gt[2 * p], gt[2 * p + 1]], axis=0)
        count = jnp.where(first_pos, lens[2 * p], lens[2 * p + 1])
        last = jnp.sum(jnp.where(pos == count - 1, g, 0.0), axis=1, keepdims=True)
        s = s + (last - g)
        scores[8 * p:8 * p + 8, :] = jnp.where(pos < count, s, -jnp.inf)
    phase("project_kv")
    ready("wk", "wv", "wf")
    key_new = dot(normed, wk[...]).astype(BF16).astype(F32)
    value_new = dot(normed, wv[...]).astype(BF16).astype(F32)
    forget = dot(normed, wf[...], NT)
    forget = jnp.minimum(forget, 0.0) - jnp.log1p(jnp.exp(-jnp.abs(forget)))
    for h in range(4):
        of_head = pl.ds(h, seqs, stride=4)
        fanned[1, of_head, :] = key_new
        fanned[2, of_head, :] = value_new
        fanned[3, of_head, :] = jnp.broadcast_to(forget[:, h:h + 1], (seqs, 128))
    phase("softmax")
    self_score = jnp.sum(fanned[0] * fanned[1], axis=1, keepdims=True)
    s = scores[...] + fanned[3][:, :1]
    peak = jnp.maximum(jnp.max(s, axis=1, keepdims=True), self_score)
    weight = jnp.exp(s - peak)
    self_weight = jnp.exp(self_score - peak)
    total = jnp.sum(weight, axis=1, keepdims=True) + self_weight
    scores[...] = weight / total
    self_prob = (self_weight / total).astype(BF16).astype(F32)
    for p in range(pairs):
        if p == 0:
            phase("v_wait0")
            v_half[0].wait()
            for item in later:
                load(*item)
            phase("values0")
        if p == pairs // 2:
            phase("v_wait1")
            v_half[1].wait()
            ready("wo")
            phase("values1")
        prob = scores[8 * p:8 * p + 8, :].astype(BF16)
        v_pair = jnp.concatenate([vc[2 * p], vc[2 * p + 1]], axis=1)
        mixed = dot(prob, v_pair)
        heads[8 * p:8 * p + 8, :] = jnp.where(first, mixed[:, :128], mixed[:, 128:])
    heads[...] = heads[...] + self_prob * fanned[2]
    a0, a1, a2, a3 = (
        heads[pl.ds(h, seqs, stride=4), :].astype(BF16).astype(F32) for h in range(4))
    attn = jnp.concatenate([
        jnp.where(low, a0, pltpu.roll(a1, 64, 1)), jnp.where(low, pltpu.roll(a2, 64, 1), a3),
    ], axis=1).astype(BF16)
    mine[...] = dot(attn, wo[...]).astype(BF16)

    phase("barrier")
    pl.semaphore_wait(barrier, half + core)

    phase("swap_start")
    sibling = (ep, 1 - core)
    swap = pltpu.make_async_remote_copy(
        mine, theirs, att_sem.at[0], att_sem.at[1], device_id=sibling, device_id_type=MESH)
    swap.start()
    ready("gain2")
    phase("swap_wait")
    swap.wait_recv()
    phase("norm2")
    residual = (
        tok[...].astype(F32) + (mine[...].astype(F32) + theirs[...].astype(F32))).astype(BF16)
    out_residual[...] = residual
    ffn_rows = norm_rows(residual.astype(F32), gain2[...].reshape(1, width))

    phase("pack")

    def landed(dz, src, dst, send, recv):
        def take(count):
            part = pl.ds(dz * block, count)
            pltpu.make_async_remote_copy(
                src.at[part], dst.at[part], send.at[0], recv.at[dz],
                device_id=sibling, device_id_type=MESH).wait_recv()

        here = jnp.logical_and(core == 0, dz == 0)
        pl.when(here)(lambda: take(block - 1) if block > 1 else None)
        pl.when(jnp.logical_not(here))(lambda: take(block))

    def go_landed(dz):
        landed(dz, box_out, box_in, go_send, go_recv)

    def back_landed(dz):
        landed(dz, ret_out, ret_in, back_send, back_recv)

    def sent(src, dst, send, recv):
        def take(count):
            part = pl.ds(0, count)
            pltpu.make_async_remote_copy(
                src.at[part], dst.at[part], send.at[0], recv.at[0],
                device_id=sibling, device_id_type=MESH).wait_send()

        pl.when(core == 0)(lambda: take(half - 1))
        pl.when(core == 1)(lambda: take(half))

    def go(dz, k):
        i = dz * block + k
        return pltpu.make_async_remote_copy(
            box_out.at[i], box_in.at[i], go_send.at[0], go_recv.at[dz],
            device_id=(peer(dz, k, True), core), device_id_type=MESH)

    def back(dz, k):
        i = dz * block + k
        return pltpu.make_async_remote_copy(
            ret_out.at[i], ret_in.at[i], back_send.at[0], back_recv.at[dz],
            device_id=(peer(dz, k, False), core), device_id_type=MESH)

    lines = [pl.ds(j, b_rows, stride=cols) for j in range(cols)]
    box_shape = (block, CAP * cols, 128)

    for dz in sorted(range(nz), key=lambda dz: (-min(dz, nz - dz), -dz)):
        chosen = pick[dz * b_rows:(dz + 1) * b_rows].astype(BF16)
        stage = lay.at[dz % z_step]
        for j in range(cols // 2):
            part = dot(chosen, ffn_rows[:, 256 * j:256 * j + 256])
            stage[lines[2 * j], :] = part[:, :128]
            stage[lines[2 * j + 1], :] = part[:, 128:]
        box_out[pl.ds(dz * block, block)] = stage[...].astype(BF16).reshape(box_shape)
        each(dz, lambda k: go(dz, k).start())

    @pl.when(core == 0)
    def _():
        box_in[block - 1] = box_out[block - 1]

    ready("eg", "eu", "ed")
    pushes = [
        pltpu.make_async_remote_copy(
            buf.at[0], buf.at[1], wt_send.at[n], wt_recv.at[n], device_id=sibling,
            device_id_type=MESH)
        for n, buf in enumerate((eg, eu, ed))
    ]
    for push in pushes:
        push.start()

    phase("shared")
    ready("rw")
    chance = dot(rw[...], ffn_rows, NT)
    chance = marks_all / (1.0 + jnp.exp(-chance))
    share = ROUTE_SCALE * chance / jnp.sum(chance, axis=0, keepdims=True)
    slot_w = dot(to_slot, share, precision=HIGH) * pick
    slot_hi = slot_w.astype(BF16).astype(F32)
    slot_w = jnp.concatenate([slot_hi, slot_w - slot_hi], axis=1)
    mix = [
        jnp.transpose(slot_w[dz * b_rows:(dz + 1) * b_rows]).astype(BF16) for dz in range(nz)
    ]
    ready("sg", "su", "sd")
    shared_h = (silu(dot(ffn_rows, sg[...])) * dot(ffn_rows, su[...])).astype(BF16)
    total_rows[...] = dot(shared_h, sd[...])

    hidden_w = eg.shape[2]
    phase("push_wait")
    for push in pushes:
        push.wait_recv()
    singles = nz - z_step
    for some_z in [[n] for n in range(singles)] + [list(range(singles, nz))]:
        first_z, count = some_z[0], len(some_z) * b_rows
        from_z = [(z + nz - n) % nz for n in some_z]
        phase(f"go_wait{first_z}")
        for dz in from_z:
            go_landed(dz)
        phase(f"unpack{first_z}")
        for n, dz in enumerate(from_z):
            lay[n] = box_in[pl.ds(dz * block, block)].reshape(b_rows * cols, 128).astype(F32)
        for j in range(cols):
            xs[:count, 128 * j:128 * j + 128] = jnp.concatenate(
                [lay.at[n][lines[j], :] for n in range(len(some_z))], axis=0).astype(BF16)
        phase(f"ffn_in{first_z}")
        for part in range(2):
            gate = dot(xs[:count], eg[part])
            up = dot(xs[:count], eu[part])
            hid[:count, hidden_w * part:hidden_w * (part + 1)] = (silu(gate) * up).astype(BF16)
        phase(f"ffn_out{first_z}")
        for j in range(cols // 2):
            down = ed[:, :, 256 * j:256 * j + 256].reshape(2 * hidden_w, 256)
            answer = dot(hid[:count], down)
            for n in range(len(some_z)):
                piece = answer[n * b_rows:(n + 1) * b_rows]
                lay.at[n][lines[2 * j], :] = piece[:, :128]
                lay.at[n][lines[2 * j + 1], :] = piece[:, 128:]
        phase(f"back_start{first_z}")
        for n, dz in enumerate(from_z):
            ret_out[pl.ds(dz * block, block)] = lay[n].astype(BF16).reshape(box_shape)
            each(dz, lambda k: back(dz, k).start())

    @pl.when(core == 0)
    def _():
        ret_in[block - 1] = ret_out[block - 1]

    lots = [list(range(z_step))] + [[dz] for dz in range(z_step, nz)]
    for m, some in enumerate(lots):
        phase(f"back_wait{m}")
        for dz in some:
            back_landed(dz)
        phase(f"combine{m}")
        for n, dz in enumerate(some):
            lay[n] = ret_in[pl.ds(dz * block, block)].reshape(b_rows * cols, 128).astype(F32)
        for j in range(cols // 2):
            span = slice(256 * j, 256 * j + 256)
            part = total_rows[:, span]
            for n, dz in enumerate(some):
                answer = jnp.concatenate(
                    [lay.at[n][lines[2 * j], :], lay.at[n][lines[2 * j + 1], :]],
                    axis=1).astype(BF16)
                both = dot(mix[dz], answer)
                part = part + (both[:seqs] + both[seqs:])
            if m + 1 < len(lots):
                total_rows[:, span] = part
            else:
                out_mine[:, span] = part.astype(BF16)

    phase("finish")
    finish = pltpu.make_async_remote_copy(
        out_mine, out_theirs, fin_sem.at[0], fin_sem.at[1], device_id=sibling,
        device_id_type=MESH)
    finish.start()
    swap.wait_send()
    for push in pushes:
        push.wait_send()
    sent(box_out, box_in, go_send, go_recv)
    sent(ret_out, ret_in, back_send, back_recv)
    finish.wait_send()
    finish.wait_recv()
    phase()


def split_dims(n):
    return {64: (4, 4, 4), 4: (1, 2, 2), 8: (2, 2, 2)}[n]


def per_device(
    tokens, norm_gain, w_query, w_key, w_value, w_forget, w_out, cache_keys, cache_values,
    cache_gates, lengths, ffn_gain, router_w, routes, shared_gate, shared_up, shared_down,
    expert_gate, expert_up, expert_down,
):
    seqs, width = tokens.shape
    n_ep = lax.axis_size("ep")
    half = n_ep // 2
    dims = split_dims(n_ep)
    z_step = min(Z_STEP, dims[0])
    step_rows = half * CAP // dims[0] * z_step
    cols = width // 128
    positions = cache_keys.shape[1]
    ff = expert_gate.shape[2]
    any_spec = pl.BlockSpec(memory_space=pl.ANY)
    operands = (
        tokens, norm_gain, w_query, w_key, w_value, w_forget.T, w_out,
        cache_keys, cache_values, cache_gates, lengths, ffn_gain, router_w.T,
        routes.T, shared_gate, shared_up, shared_down, expert_gate, expert_up, expert_down,
    )
    operands = tuple(
        pltpu.with_memory_space_constraint(operand, pltpu.HBM) for operand in operands)
    vmem = pltpu.VMEM
    dma = pltpu.SemaphoreType.DMA

    def like(index):
        return vmem(operands[index].shape, operands[index].dtype)

    scratch = [
        like(0), like(1), like(2), like(3), like(4), like(5), like(6), like(7), like(8), like(9),
        pltpu.SMEM(lengths.shape, jnp.int32), like(11), like(12), like(13), like(14), like(15),
        like(16),
        vmem((2, width, ff), BF16), vmem((2, width, ff), BF16), vmem((2, ff, width), BF16),
        vmem((4 * seqs, positions), F32), vmem((4 * seqs, 128), F32),
        vmem((4, 4 * seqs, 128), F32),
        vmem((seqs, width), BF16), vmem((seqs, width), BF16),
        vmem((step_rows, width), BF16), vmem((step_rows, 2 * ff), BF16),
        vmem((z_step, step_rows // z_step * cols, 128), F32),
        vmem((half, CAP * cols, 128), BF16), vmem((half, CAP * cols, 128), BF16),
        vmem((half, CAP * cols, 128), BF16), vmem((half, CAP * cols, 128), BF16),
        vmem((seqs, width), F32),
        dma((SLOTS,)), dma((2,)), dma((2,)), dma((2,)), dma((3,)), dma((3,)),
        dma((1,)), dma((dims[0],)), dma((1,)), dma((dims[0],)), dma((2,)),
    ]
    residual, own, other = pl.pallas_call(
        functools.partial(kernel, dims),
        out_shape=[jax.ShapeDtypeStruct((seqs, width), BF16)] * 3,
        in_specs=[any_spec] * len(operands),
        out_specs=[pl.BlockSpec(memory_space=pltpu.VMEM)] * 3,
        scratch_shapes=scratch,
        compiler_params=pltpu.CompilerParams(
            collective_id=0, has_side_effects=True, vmem_limit_bytes=32 * 1024 * 1024),
    )(*operands)
    return (residual.astype(F32) + (own.astype(F32) + other.astype(F32))).astype(BF16)


def solution(mesh):
    placed = (
        P("ep", None),
        P(),
        P(None, "tp"),
        P(None, "tp"),
        P(None, "tp"),
        P(None, "tp"),
        P("tp", None),
        P("ep", None, "tp"),
        P("ep", None, "tp"),
        P("ep", "tp", None),
        P("ep"),
        P(),
        P(),
        P("ep", None),
        P(None, "tp"),
        P(None, "tp"),
        P("tp", None),
        P("ep", None, "tp"),
        P("ep", None, "tp"),
        P("ep", "tp", None),
    )
    return jax.shard_map(
        per_device, mesh=mesh, in_specs=placed, out_specs=P("ep", None), check_vma=False
    )
```
